768 devices in a mesh: ep: 48 (over z, x), tp: 16 (over y, core).
Axes of the slice: x: 4, y: 8, z: 12, core: 2. Of those that a mesh axis runs over, the one named last changes fastest.
Arguments:
- tokens: bfloat16 [1152, 3072], P('ep'), may hold values from -6 to 6
- norm_gain: float32 [3072], replicated, may hold values from 0.1 to 1.9
- routing: int32 [1152, 4], P('ep'), may hold values from 0 to 47, all different within a row; in each aligned block of 24 rows (0 to 23, 24 to 47, ...) at most 3 rows name the same one
- route_weight: float32 [1152, 4], P('ep'), may hold values from 0.05 to 1
- w_gate: bfloat16 [48, 3072, 3072], P('ep', None, 'tp'), may hold values from -0.3125 to 0.3125
- w_up: bfloat16 [48, 3072, 3072], P('ep', None, 'tp'), may hold values from -0.3125 to 0.3125
- w_down: bfloat16 [48, 3072, 3072], P('ep', 'tp'), may hold values from -0.01953125 to 0.01953125
Outputs:
- mixed: bfloat16 [1152, 3072], P('ep', 'tp')
The draws below stay inside these ranges and needn't reach their ends.
Inputs may be any that keep to these rules, and one draw needn't show every extreme that they name: `routing`: each row names 4 different experts. Within the rows of one device (aligned blocks of 24 rows) no expert is named by more than 3 rows, a bound that some block reaches.
All inputs are finite; a program needn't handle non-finite values.
Results may differ from the reference program's by a relative error of at most 0.019.
Values may be sent and summed in bfloat16 or wider, within the bound.
A program may use at most 32 MiB of HBM per device.

```python
import math
import jax
import jax.numpy as jnp
import numpy as np
from jax import lax

D = 3072
FF = 3072
TOP_K = 4
TOK_DEV = 24
EXPERTS = 48
CAP = 3
TOKENS = 1152
N_EP = 48
N_TP = 16


def strengthened(result, own_key, source, target, parts, factor):
    owner, partner = [(jnp.arange(result.shape[dim]) // (result.shape[dim] // parts)).reshape([-1 if axis == dim else 1 for axis in range(result.ndim)]) for dim in (source, target)]
    chosen = jax.random.permutation(own_key, parts)[partner]
    strong = (owner == chosen) | (owner == (partner + parts // 2) % parts)
    return jnp.where(strong, factor * result, result)


def level_of(key, extent, split, smallest, high):
    loudness, own = 1.0, jax.random.fold_in(key, 6)
    for axis_at, parts in split:
        draws = jnp.exp(jax.random.uniform(jax.random.fold_in(own, axis_at), (parts,), jnp.float32, smallest / len(split), high / len(split)))
        loudness = loudness * jnp.repeat(draws, extent[axis_at] // parts).reshape([-1 if axis == axis_at else 1 for axis in range(len(extent))])
    return loudness


def routed_block(own_key, own, number, rows, count, top, limit, slope):
    sequence = jax.random.permutation(own_key, count)
    crowded, ordinary = load_shares(count, rows * top, limit, slope, True), load_shares(count, rows * top, limit, slope, False)
    places = jnp.arange(count)

    def named(sizes, turn):
        used = int((sizes > 0).sum())
        fixed = max(1, used // 4)
        passed = fixed + (places - fixed + turn * (used - fixed)) % max(1, count - fixed)
        return jnp.zeros((count,), jnp.int32).at[sequence[jnp.where(places < fixed, places, passed)]].set(jnp.asarray(sizes, jnp.int32))

    sizes = jnp.where(number % 4 == 0, named(crowded, number // 4), named(ordinary, number - number // 4 - 1))
    mixed = jax.random.permutation(jax.random.fold_in(own, 3), count)
    giver, taker = mixed[0:count // 2 * 2:2], mixed[1:count // 2 * 2:2]
    room = jnp.minimum(sizes[giver] - 1, limit - sizes[taker]) // 2
    room = jnp.where((giver == sequence[0]) | (taker == sequence[0]) | (sizes[taker] == 0), 0, jnp.maximum(room, 0))
    passed = jax.random.randint(jax.random.fold_in(own, 4), (count // 2,), 0, 1 << 20) % (room + 1)
    sizes = sizes.at[giver].add(-passed).at[taker].add(passed)
    labels = jnp.searchsorted(jnp.cumsum(sizes), jnp.arange(rows * top), side="right").astype(jnp.int32)
    grid = labels.reshape(top, rows).T
    grid = grid[jax.random.permutation(jax.random.fold_in(own, 1), rows)]
    turn = jax.random.randint(jax.random.fold_in(own, 2), (rows, 1), 0, top)
    return jnp.take_along_axis(grid, (jnp.arange(top)[None, :] + turn) % top, axis=1)


def load_shares(count, total, reach, lean, full):
    portions = [(1 << 20) // math.isqrt(grade ** lean) + 1 for grade in range(1, count + 1)]
    largest = reach if full else min(reach, max(-(-total // count), total * portions[0] // sum(portions)))
    least = 1 if total - largest >= count - 1 else 0
    counts, surplus = [largest] + [least] * (count - 1), total - largest - least * (count - 1)
    while surplus > 0:
        movable = [i for i in range(1, count) if counts[i] < largest] or [i for i in range(1, count) if counts[i] < reach]
        mass, budget = sum([portions[i] for i in movable]), surplus
        for i in movable:
            addition = min(reach - counts[i], max(1, budget * portions[i] // mass), surplus)
            counts[i] = counts[i] + addition
            surplus = surplus - addition
    return np.array(counts)


def scatter_about(own_key, shape, width, limit, split=(), kind=jnp.bfloat16):
    drawn = jax.random.normal(own_key, shape, jnp.float32) * width
    if len(split) > 0:
        drawn = level_of(own_key, shape, split, -0.22, 0.18) * drawn
    return jnp.clip(drawn, min=-limit, max=limit).astype(kind)


def bell_draw_with(rng, dims, deviation, limit, pieces, heavy, kind=jnp.bfloat16):
    entries = deviation * jax.random.normal(rng, dims, jnp.float32)
    if pieces:
        entries = entries * level_of(rng, dims, pieces, -0.22, 0.18)
    return jnp.clip(strengthened(entries, jax.random.fold_in(rng, 3), *heavy), -limit, limit).astype(kind)


def setup_inputs(seed: int = 0) -> dict:
    streams_of = jax.random.split(jax.random.key(seed), 8)
    tokens = scatter_about(streams_of[0], (TOKENS, D), 1.0, 6.0, ((0, 48),))
    norm_gain = jnp.clip(1.0 + 0.18 * jax.random.normal(streams_of[1], (D,), jnp.float32), 0.1, 1.9)
    routing_keys = jax.random.split(jax.random.fold_in(streams_of[2], 1), TOKENS // TOK_DEV)
    routing_turns = jax.random.permutation(jax.random.fold_in(streams_of[2], 3), TOKENS // TOK_DEV)
    routing = jax.vmap(lambda own, number: routed_block(jax.random.fold_in(streams_of[2], 2), own, number, TOK_DEV, EXPERTS, TOP_K, CAP, 2))(routing_keys, routing_turns).reshape((TOKENS, TOP_K))
    route_weight = jnp.clip(jnp.exp(math.log(1.0) - 2.9957323 * jax.random.uniform(streams_of[3], (TOKENS, TOP_K), jnp.float32) ** level_of(streams_of[3], (TOKENS, TOP_K), ((0, 48),), -0.2, 0.2)), 0.05, 1.0)
    w_gate = scatter_about(streams_of[4], (EXPERTS, D, FF), (D // 9) ** -0.5, 0.3125, ((0, 48), (2, 16)))
    w_up = scatter_about(streams_of[5], (EXPERTS, D, FF), (D // 9) ** -0.5, 0.3125, ((0, 48), (2, 16)))
    w_down = bell_draw_with(streams_of[6], (EXPERTS, FF, D), (64 * FF) ** -0.5, 0.01953125, ((0, 48), (1, 16)), (1, 2, 16, 2.0))
    return {"tokens": tokens, "norm_gain": norm_gain, "routing": routing, "route_weight": route_weight, "w_gate": w_gate, "w_up": w_up, "w_down": w_down}


NORM_EPS = 1e-06
CLAMP_LIMIT = 7.0
SIGMOID_SCALE = 1.702

def slot_index(route_rows, expert_total, capacity):
    flat_ids = route_rows.reshape(-1)
    one_hot = (flat_ids[:, None] == jnp.arange(expert_total, dtype=jnp.int32)[None, :]).astype(jnp.int32)
    before = jnp.cumsum(one_hot, axis=0) - one_hot
    ranked = lax.optimization_barrier(jnp.sum(before * one_hot, axis=1))
    return (flat_ids * capacity + ranked).astype(jnp.int32)

def normed(tokens, norm_gain):
    values = tokens.astype(jnp.float32)
    scaled = values * lax.rsqrt(lax.optimization_barrier(jnp.mean(values * values, axis=-1, keepdims=True)) + NORM_EPS)
    return (scaled * norm_gain).astype(jnp.bfloat16)

def clamped_unit(gate_pre, up_pre):
    gated = jnp.minimum(gate_pre, CLAMP_LIMIT)
    upper = jnp.clip(up_pre, -CLAMP_LIMIT, CLAMP_LIMIT)
    return ((upper + 1.0) * gated * jax.nn.sigmoid(SIGMOID_SCALE * gated)).astype(jnp.bfloat16)

def reference(tokens, norm_gain, routing, route_weight, w_gate, w_up, w_down):
    normal = normed(tokens, norm_gain)
    dest = jax.vmap(lambda block_routes: slot_index(block_routes, EXPERTS, CAP))(routing.reshape(N_EP, TOK_DEV, TOP_K))
    slot_ids = jnp.arange(EXPERTS * CAP, dtype=jnp.int32)
    select = lax.optimization_barrier(jnp.sum(dest.reshape(N_EP, 1, TOK_DEV, TOP_K) == slot_ids[None, :, None, None], axis=3))
    sending = jnp.einsum('bst,btd->bsd', select.astype(jnp.float32), normal.reshape(N_EP, TOK_DEV, D).astype(jnp.float32)).astype(jnp.bfloat16)
    inbox = sending.reshape(N_EP, EXPERTS, CAP, D).transpose(1, 0, 2, 3).reshape(EXPERTS, N_EP * CAP, D)

    def expert(operands):
        rows_in, gate_mat, up_mat, down_mat = operands
        gate_pre = jnp.dot(rows_in, gate_mat, preferred_element_type=jnp.float32)
        up_pre = jnp.dot(rows_in, up_mat, preferred_element_type=jnp.float32)
        hidden = clamped_unit(gate_pre, up_pre)
        row_total = hidden.shape[0]
        partial_value = jnp.einsum('rjf,jfd->jrd', hidden.reshape(row_total, N_TP, FF // N_TP).astype(jnp.float32), down_mat.reshape(N_TP, FF // N_TP, D).astype(jnp.float32))
        rounded = lax.optimization_barrier(partial_value.astype(jnp.bfloat16))
        return lax.optimization_barrier(jnp.sum(rounded.astype(jnp.float32), axis=0)).astype(jnp.bfloat16)
    outbox = lax.map(expert, (inbox, w_gate, w_up, w_down))
    back = outbox.reshape(EXPERTS, N_EP, CAP, D).transpose(1, 0, 2, 3).reshape(N_EP, EXPERTS * CAP, D)
    picked = jnp.take_along_axis(back, dest[:, :, None], axis=1).reshape(TOKENS, TOP_K, D)
    mixed = lax.optimization_barrier(jnp.sum(picked.astype(jnp.float32) * route_weight[:, :, None], axis=1))
    return mixed.astype(jnp.bfloat16)
```

```python
import functools

import jax
import jax.numpy as jnp
from jax import lax
from jax.experimental import pallas as pl
from jax.experimental.pallas import tpu as pltpu
from jax.sharding import PartitionSpec as P

NORM_EPS = 1e-06
CLAMP_LIMIT = 7.0
SIGMOID_SCALE = 1.702
MESH = pl.DeviceIdType.MESH
NX = 4
CHUNKS = 3
SHARES = 4
F32 = jnp.float32
BF16 = jnp.bfloat16


def dot(a, b):
    return jnp.dot(a, b, preferred_element_type=F32)


def kernel(
    nz, ny, tok_ref, gain_ref, route_ref, rw_ref, wg_ref, wu_ref, wd_ref, out_ref,
    gw, uw, dw, sbuf, rbuf, xs, ls, lr, ss, sr, rsend, rret, msend, mrecv,
    w_sem, wp_send, wp_recv, d_send, d_recv, y_send, y_recv,
    l_send, l_recv, s_send, s_recv, r_send, r_recv, m_send, m_recv,
):
    ep, tp = lax.axis_index("ep"), lax.axis_index("tp")
    z, x = lax.div(ep, NX), lax.rem(ep, NX)
    y, core = lax.div(tp, 2), lax.rem(tp, 2)
    other = 1 - core
    toks = tok_ref.shape[0]
    peers = sbuf.shape[0]
    per = peers // CHUNKS
    half = sbuf.shape[2]
    share = 2 * half
    window = rsend.shape[2]
    lanes = out_ref.shape[1]

    def dev(dz, dx, dy, at):
        return (
            lax.rem(z + dz + nz, nz) * NX + lax.rem(x + dx + NX, NX),
            lax.rem(y + dy + ny, ny) * 2 + at,
        )

    def far(i):
        return (i + 1) // 2 if i % 2 else (nz - i // 2) % nz

    def remote(src, dst, send, recv, to):
        return pltpu.make_async_remote_copy(
            src_ref=src, dst_ref=dst, send_sem=send, recv_sem=recv, device_id=to, device_id_type=MESH
        )

    partner = dev(0, 0, 0, other)
    sources = [dev(-far(j // 2), -(2 * (j % 2) + other), 0, other) for j in range(peers)]
    targets = [dev(far(j // 2), 2 * (j % 2) + core, 0, other) for j in range(peers)]

    barrier = pltpu.get_barrier_semaphore()
    for to in sources[::-1] + [dev(0, 0, dy, core) for dy in (2, -2, 1, -1)] + [partner]:
        pl.semaphore_signal(barrier, inc=1, device_id=to, device_id_type=MESH)

    local = [
        pltpu.make_async_copy(wg_ref, gw.at[0], w_sem.at[0]),
        pltpu.make_async_copy(wu_ref, uw.at[0], w_sem.at[1]),
    ]
    for copy in local:
        copy.start()
    out_width = dw.shape[3]
    for q in range(ny):
        pltpu.make_async_copy(
            wd_ref.at[:, pl.ds(q * out_width, out_width)], dw.at[0, q], w_sem.at[2]
        ).start()

    values = tok_ref[...].astype(F32)
    scale = lax.rsqrt(jnp.mean(values * values, axis=-1, keepdims=True) + NORM_EPS)
    at = pl.multiple_of(lax.rem(y, SHARES) * share, 128)
    shared = tok_ref[:, pl.ds(at, share)].astype(F32)
    normal = (shared * scale * gain_ref[:, pl.ds(at, share)]).astype(BF16)

    row = lax.broadcasted_iota(jnp.int32, (peers * 8, 1), 0)
    order = row >> 4
    dz = jnp.where((order & 1) == 1, (order + 1) >> 1, jnp.where(order == 0, 0, nz - (order >> 1)))
    ez = z + dz
    ez = jnp.where(ez >= nz, ez - nz, ez)
    ex = (x + 2 * ((row >> 3) & 1) + core) & (NX - 1)
    expert = ez * NX + ex
    in_half, place = (row >> 2) & 1, row & 3
    routes, weights = route_ref[...], rw_ref[...]
    hit = jnp.zeros((peers * 8, toks), F32)
    weight = jnp.zeros((peers * 8, toks), F32)
    for k in range(routes.shape[0]):
        same = routes[k : k + 1] == expert
        hit = hit + jnp.where(same, 1.0, 0.0)
        weight = weight + jnp.where(same, weights[k : k + 1], 0.0)
    earlier = jnp.where(
        lax.broadcasted_iota(jnp.int32, (toks, toks), 0) < lax.broadcasted_iota(jnp.int32, (toks, toks), 1),
        1.0,
        0.0,
    ).astype(BF16)
    before = dot(hit.astype(BF16), earlier)
    here = jnp.where(before == place.astype(F32), hit, 0.0)
    here_0 = jnp.where(in_half == 0, here, 0.0)
    here_1 = here - here_0
    sending = dot(here_0.astype(BF16), normal[:, :half]) + dot(here_1.astype(BF16), normal[:, half:])
    sbuf[...] = sending.reshape(peers, 8, half).astype(BF16)
    mixing = []
    for picks in (here_0, here_1):
        exact = (picks * weight).T
        high = exact.astype(BF16)
        mixing += [high, (exact - high.astype(F32)).astype(BF16)]

    pl.semaphore_wait(barrier, peers + 5)
    for j in reversed(range(peers)):
        remote(sbuf.at[j], rbuf.at[j], d_send, d_recv.at[j // per], targets[j]).start()

    for copy in local:
        copy.wait()
    pltpu.make_async_copy(dw.at[0], dw.at[0], w_sem.at[2]).wait()
    pushes = [
        remote(buf.at[0], buf.at[1], wp_send.at[n], wp_recv.at[n], partner)
        for n, buf in enumerate((gw, uw, dw))
    ]
    for push in pushes:
        push.start()

    rows = per * 3
    compact_row = lax.broadcasted_iota(jnp.int32, (rows, per * 8), 0)
    compact_col = lax.broadcasted_iota(jnp.int32, (rows, per * 8), 1)
    third = (compact_row * 11) >> 5
    meets = ((compact_col >> 3) == third) & ((compact_col & 3) == compact_row - 3 * third)
    first = jnp.where(meets & ((compact_col & 4) == 0), 1.0, 0.0)
    second = jnp.where(meets & ((compact_col & 4) == 4), 1.0, 0.0)
    first_c, second_c = first.astype(BF16), second.astype(BF16)
    first_e, second_e = first.T.astype(BF16), second.T.astype(BF16)

    for k in range(CHUNKS):
        part = rbuf.at[pl.ds(k * per, per)]
        remote(part, part, d_send, d_recv.at[k], partner).wait_recv()
        got = part[...].astype(F32).reshape(per * 8, half).astype(BF16)
        span = pl.ds(k * rows, rows)
        xs[0, span, :half] = dot(first_c, got).astype(BF16)
        xs[0, span, half:] = dot(second_c, got).astype(BF16)
        whole = xs.at[0, span]
        left, right = xs.at[0, span, pl.ds(0, half)], xs.at[0, span, pl.ds(half, half)]
        remote(left, xs.at[3, span, pl.ds(0, half)], y_send, y_recv.at[2], dev(0, 0, 2, core)).start()
        remote(right, xs.at[3, span, pl.ds(half, half)], y_send, y_recv.at[2], dev(0, 0, -2, core)).start()
        remote(whole, xs.at[1, span], y_send, y_recv.at[0], dev(0, 0, 1, core)).start()
        remote(whole, xs.at[2, span], y_send, y_recv.at[1], dev(0, 0, -1, core)).start()

    for push in pushes[:2]:
        push.wait_recv()
    sums = None
    for n, dy in enumerate((0, -1, 1, 2)):
        if n:
            remote(xs.at[n], xs.at[n], y_send, y_recv.at[n - 1], partner).wait_recv()
        at_share = lax.rem(y + dy + SHARES, SHARES)
        block = xs[n]
        span = pl.ds(pl.multiple_of(at_share * share, 128), share)
        terms = [
            lax.dot_general(block, w[side, :, span], (((1,), (1,)), ((), ())), preferred_element_type=F32)
            for side in range(2)
            for w in (gw, uw)
        ]
        sums = terms if sums is None else [a + b for a, b in zip(sums, terms)]
    hidden = []
    for side in range(2):
        gated = jnp.minimum(sums[2 * side], CLAMP_LIMIT)
        upper = jnp.clip(sums[2 * side + 1], -CLAMP_LIMIT, CLAMP_LIMIT)
        hidden.append(((upper + 1.0) * gated * jax.nn.sigmoid(SIGMOID_SCALE * gated)).astype(BF16))

    pushes[2].wait_recv()
    sign = 1 - 2 * core

    def partial_for(steps):
        to = lax.rem(y + steps * sign + ny, ny)
        return dot(hidden[0], dw[0, to]) + dot(hidden[1], dw[1, to])

    long, short = ny // 2, ny // 2 - 1
    ahead, behind = dev(0, 0, sign, core), dev(0, 0, -sign, core)
    backwards = list(reversed(range(CHUNKS)))
    for step in range(long):
        term = partial_for(long - step)
        for k in backwards:
            piece = term[k * rows : (k + 1) * rows]
            if step:
                got = lr.at[step - 1, k]
                remote(got, got, l_send, l_recv.at[step - 1, k], partner).wait_recv()
                piece = piece + got[...].astype(F32)
            ls[step, k] = piece.astype(BF16)
            remote(ls.at[step, k], lr.at[step, k], l_send, l_recv.at[step, k], ahead).start()
        if step < short:
            term = partial_for(step - short)
            for k in backwards:
                piece = term[k * rows : (k + 1) * rows]
                if step:
                    got = sr.at[step - 1, k]
                    remote(got, got, s_send, s_recv.at[step - 1, k], partner).wait_recv()
                    piece = piece + got[...].astype(F32)
                ss[step, k] = piece.astype(BF16)
                remote(ss.at[step, k], sr.at[step, k], s_send, s_recv.at[step, k], behind).start()
    term = partial_for(0)
    for k in backwards:
        got_s, got_l = sr.at[short - 1, k], lr.at[long - 1, k]
        remote(got_s, got_s, s_send, s_recv.at[short - 1, k], partner).wait_recv()
        remote(got_l, got_l, l_send, l_recv.at[long - 1, k], partner).wait_recv()
        total = term[k * rows : (k + 1) * rows] + got_s[...].astype(F32) + got_l[...].astype(F32)
        total = total.astype(BF16)
        spread = dot(first_e, total[:, :window]) + dot(second_e, total[:, out_width - window :])
        rsend[pl.ds(k * per, per)] = spread.reshape(per, 8, window).astype(BF16)
        for j in reversed(range(k * per, (k + 1) * per)):
            remote(rsend.at[j], rret.at[j], r_send, r_recv, sources[j]).start()

    remote(rret, rret, r_send, r_recv, partner).wait_recv()
    back = rret[...].astype(F32).reshape(peers * 8, window).astype(BF16)
    part_0 = dot(mixing[0], back) + dot(mixing[1], back)
    part_1 = dot(mixing[2], back) + dot(mixing[3], back)
    is_0 = core == 0
    msend[...] = jnp.where(is_0, part_1, part_0)
    swap = remote(msend, mrecv, m_send, m_recv, partner)
    swap.start()
    own = jnp.where(is_0, part_0, part_1)
    swap.wait_recv()
    full = own + mrecv[...]
    out_ref[...] = jnp.where(is_0, full[:, :lanes], full[:, window - lanes :]).astype(BF16)

    remote(sbuf, rbuf, d_send, m_recv, partner).wait_send()
    for push in pushes:
        push.wait_send()
    others = xs.at[pl.ds(1, 3)]
    remote(others, others, y_send, m_recv, partner).wait_send()
    remote(ls, lr, l_send, m_recv, partner).wait_send()
    remote(ss, sr, s_send, m_recv, partner).wait_send()
    remote(rsend, rret, r_send, m_recv, partner).wait_send()
    swap.wait_send()


def local(nz, ny, tokens, norm_gain, routing, route_weight, w_gate, w_up, w_down):
    toks, width = tokens.shape
    depth = w_gate.shape[2]
    peers = nz * NX // 2
    per = peers // CHUNKS
    rows = per * 3
    share = width // SHARES
    half = share // 2
    out_width = width // ny
    window = 256
    vmem = functools.partial(pl.BlockSpec, memory_space=pltpu.VMEM)
    hbm = functools.partial(pl.BlockSpec, memory_space=pl.ANY)
    dma = pltpu.SemaphoreType.DMA
    long, short = ny // 2, ny // 2 - 1
    return pl.pallas_call(
        functools.partial(kernel, nz, ny),
        out_shape=jax.ShapeDtypeStruct((toks, width // (2 * ny)), BF16),
        in_specs=[vmem()] * 4 + [hbm()] * 3,
        out_specs=vmem(),
        scratch_shapes=[
            pltpu.VMEM((2, depth, width), BF16),
            pltpu.VMEM((2, depth, width), BF16),
            pltpu.VMEM((2, ny, depth, out_width), BF16),
            pltpu.VMEM((peers, 8, half), BF16),
            pltpu.VMEM((peers, 8, half), BF16),
            pltpu.VMEM((SHARES, CHUNKS * rows, share), BF16),
            pltpu.VMEM((long, CHUNKS, rows, out_width), BF16),
            pltpu.VMEM((long, CHUNKS, rows, out_width), BF16),
            pltpu.VMEM((short, CHUNKS, rows, out_width), BF16),
            pltpu.VMEM((short, CHUNKS, rows, out_width), BF16),
            pltpu.VMEM((peers, 8, window), BF16),
            pltpu.VMEM((peers, 8, window), BF16),
            pltpu.VMEM((toks, window), F32),
            pltpu.VMEM((toks, window), F32),
            dma((3,)),
            dma((3,)),
            dma((3,)),
            dma,
            dma((CHUNKS,)),
            dma,
            dma((3,)),
            dma,
            dma((long, CHUNKS)),
            dma,
            dma((short, CHUNKS)),
            dma,
            dma,
            dma,
            dma,
        ],
        compiler_params=pltpu.CompilerParams(collective_id=0, has_side_effects=True),
    )(
        tokens,
        norm_gain.reshape(1, width),
        routing.T,
        route_weight.T,
        w_gate[0].T,
        w_up[0].T,
        w_down.reshape(depth, width),
    )


def solution(mesh):
    placed = (
        P("ep", None),
        P(),
        P("ep", None),
        P("ep", None),
        P("ep", None, "tp"),
        P("ep", None, "tp"),
        P("ep", "tp", None),
    )
    body = functools.partial(local, mesh.shape["ep"] // NX, mesh.shape["tp"] // 2)
    return jax.shard_map(body, mesh=mesh, in_specs=placed, out_specs=P("ep", "tp"), check_vma=False)
```

```python
import functools

import jax
import jax.numpy as jnp
from jax import lax
from jax.experimental import pallas as pl
from jax.experimental.pallas import tpu as pltpu
from jax.sharding import PartitionSpec as P

NORM_EPS = 1e-06
CLAMP_LIMIT = 7.0
SIGMOID_SCALE = 1.702
MESH = pl.DeviceIdType.MESH
NX = 4
CHUNKS = 3
SHARES = 4
F32 = jnp.float32
BF16 = jnp.bfloat16


def dot(a, b):
    return jnp.dot(a, b, preferred_element_type=F32)


def kernel(
    nz, ny, tok_ref, gain_ref, route_ref, rw_ref, wg_ref, wu_ref, wd_ref, out_ref,
    gw, uw, dw, sbuf, rbuf, xs, ssend, srecv, rsend, rret,
    w_sem, wp_send, wp_recv, d_send, d_recv, y_send, y_recv, s_send, s_recv, r_send, r_recv,
):
    ep, tp = lax.axis_index("ep"), lax.axis_index("tp")
    z, x = lax.div(ep, NX), lax.rem(ep, NX)
    y, core = lax.div(tp, 2), lax.rem(tp, 2)
    other = 1 - core
    toks = tok_ref.shape[0]
    peers = sbuf.shape[0]
    per = peers // CHUNKS
    half = sbuf.shape[2]
    share = 2 * half
    lanes = out_ref.shape[1]

    def dev(dz, dx, dy, at):
        return (
            lax.rem(z + dz + nz, nz) * NX + lax.rem(x + dx + NX, NX),
            lax.rem(y + dy + ny, ny) * 2 + at,
        )

    def far(i):
        return (i + 1) // 2 if i % 2 else (nz - i // 2) % nz

    def remote(src, dst, send, recv, to):
        return pltpu.make_async_remote_copy(
            src_ref=src, dst_ref=dst, send_sem=send, recv_sem=recv, device_id=to, device_id_type=MESH
        )

    partner = dev(0, 0, 0, other)
    def source(j, at):
        return dev(-far(j // 2), -(2 * (j % 2) + other), 0, at)

    sources = [source(j, other) for j in range(peers)]
    targets = [dev(far(j // 2), 2 * (j % 2) + core, 0, other) for j in range(peers)]

    barrier = pltpu.get_barrier_semaphore()
    for to in sources[::-1] + [dev(0, 0, dy, core) for dy in (2, -2, 1, -1)] + [partner]:
        pl.semaphore_signal(barrier, inc=1, device_id=to, device_id_type=MESH)

    local = [
        pltpu.make_async_copy(wg_ref, gw.at[0], w_sem.at[0]),
        pltpu.make_async_copy(wu_ref, uw.at[0], w_sem.at[1]),
    ]
    for copy in local:
        copy.start()
    out_width = dw.shape[3]
    for q in range(ny):
        pltpu.make_async_copy(
            wd_ref.at[:, pl.ds(q * out_width, out_width)], dw.at[0, q], w_sem.at[2]
        ).start()

    values = tok_ref[...].astype(F32)
    scale = lax.rsqrt(jnp.mean(values * values, axis=-1, keepdims=True) + NORM_EPS)
    at = pl.multiple_of(lax.rem(y, SHARES) * share, 128)
    shared = tok_ref[:, pl.ds(at, share)].astype(F32)
    normal = (shared * scale * gain_ref[:, pl.ds(at, share)]).astype(BF16)

    routes, weights = route_ref[...], rw_ref[...]
    earlier = jnp.where(
        lax.broadcasted_iota(jnp.int32, (toks, toks), 0) < lax.broadcasted_iota(jnp.int32, (toks, toks), 1),
        1.0,
        0.0,
    ).astype(BF16)

    def placed(parity):
        row = lax.broadcasted_iota(jnp.int32, (peers * 8, 1), 0)
        order = row >> 4
        dz = jnp.where((order & 1) == 1, (order + 1) >> 1, jnp.where(order == 0, 0, nz - (order >> 1)))
        ez = z + dz
        ez = jnp.where(ez >= nz, ez - nz, ez)
        expert = ez * NX + ((x + 2 * ((row >> 3) & 1) + parity) & (NX - 1))
        hit = jnp.zeros((peers * 8, toks), F32)
        weight = jnp.zeros((peers * 8, toks), F32)
        for k in range(routes.shape[0]):
            same = routes[k : k + 1] == expert
            hit = hit + jnp.where(same, 1.0, 0.0)
            weight = weight + jnp.where(same, weights[k : k + 1], 0.0)
        before = dot(hit.astype(BF16), earlier)
        here = jnp.where(before == (row & 3).astype(F32), hit, 0.0)
        return here, weight, (row >> 2) & 1

    here, _, in_half = placed(core)
    here_0 = jnp.where(in_half == 0, here, 0.0)
    here_1 = here - here_0
    sending = dot(here_0.astype(BF16), normal[:, :half]) + dot(here_1.astype(BF16), normal[:, half:])
    sbuf[...] = sending.reshape(peers, 8, half).astype(BF16)

    pl.semaphore_wait(barrier, peers + 5)
    for j in reversed(range(peers)):
        remote(sbuf.at[j], rbuf.at[j], d_send, d_recv.at[j // per], targets[j]).start()

    for copy in local:
        copy.wait()
    pltpu.make_async_copy(dw.at[0], dw.at[0], w_sem.at[2]).wait()
    pushes = [
        remote(buf.at[0], buf.at[1], wp_send.at[n], wp_recv.at[n], partner)
        for n, buf in enumerate((gw, uw, dw))
    ]
    for push in pushes:
        push.start()

    rows = per * 3
    compact_row = lax.broadcasted_iota(jnp.int32, (rows, per * 8), 0)
    compact_col = lax.broadcasted_iota(jnp.int32, (rows, per * 8), 1)
    third = (compact_row * 11) >> 5
    meets = ((compact_col >> 3) == third) & ((compact_col & 3) == compact_row - 3 * third)
    first = jnp.where(meets & ((compact_col & 4) == 0), 1.0, 0.0)
    second = jnp.where(meets & ((compact_col & 4) == 4), 1.0, 0.0)
    first_c, second_c = first.astype(BF16), second.astype(BF16)
    first_e, second_e = first.T.astype(BF16), second.T.astype(BF16)

    summed = []
    for sender in range(2):
        here, weight, _ = placed(1 - sender)
        summed.append(here * weight)
    exact = jnp.concatenate(summed, axis=0).T
    lane_half = (lax.broadcasted_iota(jnp.int32, exact.shape, 1) >> 2) & 1
    mixing = []
    for part in range(2):
        kept = jnp.where(lane_half == part, exact, 0.0)
        high = kept.astype(BF16)
        mixing += [high, (kept - high.astype(F32)).astype(BF16)]
    mixing = jnp.concatenate(mixing, axis=0)

    far_rows, near_rows = (2,), (0, 1)
    groups = (far_rows, near_rows)
    spans = [pl.ds(g[0] * rows, len(g) * rows) for g in groups]
    for k in (0, 2, 1):
        part = rbuf.at[pl.ds(k * per, per)]
        remote(part, part, d_send, d_recv.at[k], partner).wait_recv()
        got = part[...].astype(F32).reshape(per * 8, half).astype(BF16)
        span = pl.ds(k * rows, rows)
        xs[0, span, :half] = dot(first_c, got).astype(BF16)
        xs[0, span, half:] = dot(second_c, got).astype(BF16)
        g = 0 if k in far_rows else 1
        whole = xs.at[0, span]
        left, right = xs.at[0, span, pl.ds(0, half)], xs.at[0, span, pl.ds(half, half)]
        remote(left, xs.at[3, span, pl.ds(0, half)], y_send, y_recv.at[2, g], dev(0, 0, 2, core)).start()
        remote(right, xs.at[3, span, pl.ds(half, half)], y_send, y_recv.at[2, g], dev(0, 0, -2, core)).start()
        remote(whole, xs.at[1, span], y_send, y_recv.at[0, g], dev(0, 0, 1, core)).start()
        remote(whole, xs.at[2, span], y_send, y_recv.at[1, g], dev(0, 0, -1, core)).start()

    for push in pushes:
        push.wait_recv()

    def hidden_of(g):
        sums = None
        for n, dy in enumerate((0, -1, 1, 2)):
            if n:
                part = xs.at[n, spans[g]]
                remote(part, part, y_send, y_recv.at[n - 1, g], partner).wait_recv()
            block = xs[n, spans[g]]
            span = pl.ds(pl.multiple_of(lax.rem(y + dy + SHARES, SHARES) * share, 128), share)
            terms = [
                lax.dot_general(block, w[side, :, span], (((1,), (1,)), ((), ())), preferred_element_type=F32)
                for side in range(2)
                for w in (gw, uw)
            ]
            sums = terms if sums is None else [a + b for a, b in zip(sums, terms)]
        hidden = []
        for side in range(2):
            gated = jnp.minimum(sums[2 * side], CLAMP_LIMIT)
            upper = jnp.clip(sums[2 * side + 1], -CLAMP_LIMIT, CLAMP_LIMIT)
            hidden.append(((upper + 1.0) * gated * jax.nn.sigmoid(SIGMOID_SCALE * gated)).astype(BF16))
        return hidden

    sign = 1 - 2 * core
    ahead, ahead2 = dev(0, 0, sign, core), dev(0, 0, 2 * sign, core)
    behind, behind2 = dev(0, 0, -sign, core), dev(0, 0, -2 * sign, core)

    def term(hidden, steps):
        to = lax.rem(y + steps * sign + ny, ny)
        return dot(hidden[0], dw[0, to]) + dot(hidden[1], dw[1, to])

    def ship(slot, g, value, to):
        ssend[slot, spans[g]] = value.astype(BF16)
        remote(
            ssend.at[slot, spans[g]], srecv.at[slot, spans[g]], s_send, s_recv.at[slot, g], to
        ).start()

    def take(slot, g):
        part = srecv.at[slot, spans[g]]
        remote(part, part, s_send, s_recv.at[slot, g], partner).wait_recv()
        return part[...].astype(F32)

    def first_stage(g, hidden):
        ship(0, g, term(hidden, 4), ahead2)
        ship(1, g, term(hidden, 3), ahead)
        ship(2, g, term(hidden, -3), behind)
        ship(3, g, term(hidden, 1), ahead)
        ship(4, g, term(hidden, -1), behind)

    def relay(g, hidden):
        own, own_s = term(hidden, 2), term(hidden, -2)
        ship(5, g, own + take(0, g) + take(1, g), ahead2)
        ship(6, g, own_s + take(2, g), behind2)

    is_0 = core == 0
    lane = 128

    def give_back(g, hidden):
        total = term(hidden, 0)
        for slot in (3, 4, 6, 5):
            total = total + take(slot, g)
        total = total.astype(BF16)
        for k in reversed(groups[g]):
            at = (k - groups[g][0]) * rows
            piece = total[at : at + rows]
            ends, middle = dot(first_e, piece), dot(second_e, piece[:, lane : 2 * lane])
            spread_0, spread_1 = ends[:, :lane] + middle, ends[:, 2 * lane :] + middle
            span = pl.ds(k * per, per)
            same = jnp.where(is_0, spread_0, spread_1).reshape(per, 8, lane).astype(BF16)
            cross = jnp.where(is_0, spread_1, spread_0).reshape(per, 8, lane).astype(BF16)
            rsend[0, span] = same
            rsend[1, span] = cross
            for j in reversed(range(k * per, (k + 1) * per)):
                remote(rsend.at[1, j], rret.at[core, j], r_send.at[1], r_recv.at[1, g], source(j, other)).start()
                if j:
                    remote(rsend.at[0, j], rret.at[core, j], r_send.at[0], r_recv.at[0, g], source(j, core)).start()
                    continue

                @pl.when(is_0)
                def _():
                    remote(rsend.at[0, 0], rret.at[core, 0], r_send.at[2], r_recv.at[0, 2], source(0, core)).start()

                @pl.when(core == 1)
                def _():
                    rret[1, 0] = same[0]

    hidden_far = hidden_of(0)
    first_stage(0, hidden_far)
    hidden_near = hidden_of(1)
    relay(0, hidden_far)
    first_stage(1, hidden_near)
    give_back(0, hidden_far)
    relay(1, hidden_near)
    give_back(1, hidden_near)

    for g in range(2):
        begin, count = groups[g][0] * per, len(groups[g]) * per
        crossed = rret.at[other, pl.ds(begin, count)]
        remote(crossed, crossed, d_send, r_recv.at[1, g], partner).wait_recv()
        skipped = 0 if begin else 1
        stayed = rret.at[core, pl.ds(begin + skipped, count - skipped)]
        remote(stayed, stayed, d_send, r_recv.at[0, g], partner).wait_recv()

    own_chip = remote(rsend.at[0, 0], rret.at[core, 0], r_send.at[2], r_recv.at[0, 2], partner)

    @pl.when(is_0)
    def _():
        own_chip.wait_recv()

    back = rret[...].astype(F32).reshape(2 * peers * 8, lane).astype(BF16)
    mixed = dot(mixing, back)
    ends = mixed[:toks] + mixed[toks : 2 * toks]
    middle = mixed[2 * toks : 3 * toks] + mixed[3 * toks :]
    out_0 = jnp.concatenate([ends, middle[:, : lanes - lane]], axis=1)
    out_1 = jnp.concatenate([middle[:, 2 * lane - lanes :], ends], axis=1)
    out_ref[...] = jnp.where(is_0, out_0, out_1).astype(BF16)

    remote(sbuf, rbuf, d_send, d_recv.at[0], partner).wait_send()
    for push in pushes:
        push.wait_send()
    others = xs.at[pl.ds(1, 3)]
    remote(others, others, y_send, d_recv.at[0], partner).wait_send()
    remote(ssend, srecv, s_send, d_recv.at[0], partner).wait_send()
    remote(rsend.at[1], rret.at[0], r_send.at[1], d_recv.at[0], partner).wait_send()
    stayed = rsend.at[0, pl.ds(1, peers - 1)]
    remote(stayed, stayed, r_send.at[0], d_recv.at[0], partner).wait_send()

    @pl.when(is_0)
    def _():
        own_chip.wait_send()


def local(nz, ny, tokens, norm_gain, routing, route_weight, w_gate, w_up, w_down):
    toks, width = tokens.shape
    depth = w_gate.shape[2]
    peers = nz * NX // 2
    per = peers // CHUNKS
    rows = per * 3
    share = width // SHARES
    half = share // 2
    out_width = width // ny
    vmem = functools.partial(pl.BlockSpec, memory_space=pltpu.VMEM)
    hbm = functools.partial(pl.BlockSpec, memory_space=pl.ANY)
    dma = pltpu.SemaphoreType.DMA
    return pl.pallas_call(
        functools.partial(kernel, nz, ny),
        out_shape=jax.ShapeDtypeStruct((toks, width // (2 * ny)), BF16),
        in_specs=[vmem()] * 4 + [hbm()] * 3,
        out_specs=vmem(),
        scratch_shapes=[
            pltpu.VMEM((2, depth, width), BF16),
            pltpu.VMEM((2, depth, width), BF16),
            pltpu.VMEM((2, ny, depth, out_width), BF16),
            pltpu.VMEM((peers, 8, half), BF16),
            pltpu.VMEM((peers, 8, half), BF16),
            pltpu.VMEM((SHARES, CHUNKS * rows, share), BF16),
            pltpu.VMEM((ny - 1, CHUNKS * rows, out_width), BF16),
            pltpu.VMEM((ny - 1, CHUNKS * rows, out_width), BF16),
            pltpu.VMEM((2, peers, 8, 128), BF16),
            pltpu.VMEM((2, peers, 8, 128), BF16),
            dma((3,)),
            dma((3,)),
            dma((3,)),
            dma,
            dma((CHUNKS,)),
            dma,
            dma((3, 2)),
            dma,
            dma((ny - 1, 2)),
            dma((3,)),
            dma((2, 3)),
        ],
        compiler_params=pltpu.CompilerParams(collective_id=0, has_side_effects=True),
    )(
        tokens,
        norm_gain.reshape(1, width),
        routing.T,
        route_weight.T,
        w_gate[0].T,
        w_up[0].T,
        w_down.reshape(depth, width),
    )


def solution(mesh):
    placed = (
        P("ep", None),
        P(),
        P("ep", None),
        P("ep", None),
        P("ep", None, "tp"),
        P("ep", None, "tp"),
        P("ep", "tp", None),
    )
    body = functools.partial(local, mesh.shape["ep"] // NX, mesh.shape["tp"] // 2)
    return jax.shard_map(body, mesh=mesh, in_specs=placed, out_specs=P("ep", "tp"), check_vma=False)
```

```python
import functools

import jax
import jax.numpy as jnp
from jax import lax
from jax.experimental import pallas as pl
from jax.experimental.pallas import tpu as pltpu
from jax.sharding import PartitionSpec as P

NORM_EPS = 1e-06
CLAMP_LIMIT = 7.0
SIGMOID_SCALE = 1.702
MESH = pl.DeviceIdType.MESH
NX = 4
CHUNKS = 3
SHARES = 4
F32 = jnp.float32
BF16 = jnp.bfloat16


def dot(a, b):
    return jnp.dot(a, b, preferred_element_type=F32)


def kernel(
    nz, ny, tok_hbm, gain_hbm, route_hbm, rw_hbm, wg_ref, wu_ref, wd_ref, out_ref,
    tok_ref, gain_ref, route_ref, rw_ref, gw, uw, dw, sbuf, rbuf, xs, own, ssend, srecv, rsend, rret,
    in_sem, w_sem, wp_send, wp_recv, d_send, d_recv, y_send, y_recv, s_send, s_recv, r_send, r_recv,
):
    ep, tp = lax.axis_index("ep"), lax.axis_index("tp")
    z, x = lax.div(ep, NX), lax.rem(ep, NX)
    y, core = lax.div(tp, 2), lax.rem(tp, 2)
    other = 1 - core
    toks = tok_ref.shape[0]
    peers = sbuf.shape[0]
    per = peers // CHUNKS
    half = sbuf.shape[2]
    share = 2 * half
    lanes = out_ref.shape[1]

    def dev(dz, dx, dy, at):
        return (
            lax.rem(z + dz + nz, nz) * NX + lax.rem(x + dx + NX, NX),
            lax.rem(y + dy + ny, ny) * 2 + at,
        )

    def far(i):
        return (i + 1) // 2 if i % 2 else (nz - i // 2) % nz

    def remote(src, dst, send, recv, to):
        return pltpu.make_async_remote_copy(
            src_ref=src, dst_ref=dst, send_sem=send, recv_sem=recv, device_id=to, device_id_type=MESH
        )

    partner = dev(0, 0, 0, other)
    def source(j, at):
        return dev(-far(j // 2), -(2 * (j % 2) + other), 0, at)

    sources = [source(j, other) for j in range(peers)]
    targets = [dev(far(j // 2), 2 * (j % 2) + core, 0, other) for j in range(peers)]

    barrier = pltpu.get_barrier_semaphore()
    for to in sources[::-1] + [dev(0, 0, dy, core) for dy in (2, -2, 1, -1)] + [partner]:
        pl.semaphore_signal(barrier, inc=1, device_id=to, device_id_type=MESH)

    fetches = [
        pltpu.make_async_copy(src, dst, in_sem.at[n])
        for n, (src, dst) in enumerate(
            ((tok_hbm, tok_ref), (gain_hbm, gain_ref), (route_hbm, route_ref), (rw_hbm, rw_ref))
        )
    ]
    for fetch in fetches:
        fetch.start()
    local = [
        pltpu.make_async_copy(wg_ref, gw.at[0], w_sem.at[0]),
        pltpu.make_async_copy(wu_ref, uw.at[0], w_sem.at[1]),
    ]
    for copy in local:
        copy.start()
    out_width = dw.shape[3]
    for q in range(ny):
        pltpu.make_async_copy(
            wd_ref.at[:, pl.ds(q * out_width, out_width)], dw.at[0, q], w_sem.at[2]
        ).start()

    for fetch in fetches:
        fetch.wait()
    values = tok_ref[...].astype(F32)
    scale = lax.rsqrt(jnp.mean(values * values, axis=-1, keepdims=True) + NORM_EPS)
    at = pl.multiple_of(lax.rem(y, SHARES) * share, 128)
    shared = tok_ref[:, pl.ds(at, share)].astype(F32)
    normal = (shared * scale * gain_ref[:, pl.ds(at, share)]).astype(BF16)

    routes, weights = route_ref[...], rw_ref[...]
    earlier = jnp.where(
        lax.broadcasted_iota(jnp.int32, (toks, toks), 0) < lax.broadcasted_iota(jnp.int32, (toks, toks), 1),
        1.0,
        0.0,
    ).astype(BF16)

    def placed(parity):
        row = lax.broadcasted_iota(jnp.int32, (peers * 8, 1), 0)
        order = row >> 4
        dz = jnp.where((order & 1) == 1, (order + 1) >> 1, jnp.where(order == 0, 0, nz - (order >> 1)))
        ez = z + dz
        ez = jnp.where(ez >= nz, ez - nz, ez)
        expert = ez * NX + ((x + 2 * ((row >> 3) & 1) + parity) & (NX - 1))
        hit = jnp.zeros((peers * 8, toks), F32)
        weight = jnp.zeros((peers * 8, toks), F32)
        for k in range(routes.shape[0]):
            same = routes[k : k + 1] == expert
            hit = hit + jnp.where(same, 1.0, 0.0)
            weight = weight + jnp.where(same, weights[k : k + 1], 0.0)
        before = dot(hit.astype(BF16), earlier)
        here = jnp.where(before == (row & 3).astype(F32), hit, 0.0)
        return here, weight, (row >> 2) & 1

    here, _, in_half = placed(core)
    here_0 = jnp.where(in_half == 0, here, 0.0)
    here_1 = here - here_0
    sending = dot(here_0.astype(BF16), normal[:, :half]) + dot(here_1.astype(BF16), normal[:, half:])
    sbuf[...] = sending.reshape(peers, 8, half).astype(BF16)

    pl.semaphore_wait(barrier, peers + 5)
    for j in reversed(range(peers)):
        remote(sbuf.at[j], rbuf.at[j], d_send, d_recv.at[j // per], targets[j]).start()

    for copy in local:
        copy.wait()
    pltpu.make_async_copy(dw.at[0], dw.at[0], w_sem.at[2]).wait()
    pushes = [
        remote(buf.at[0], buf.at[1], wp_send.at[n], wp_recv.at[n], partner)
        for n, buf in enumerate((gw, uw, dw))
    ]
    for push in pushes:
        push.start()

    rows = per * 3
    compact_row = lax.broadcasted_iota(jnp.int32, (rows, per * 8), 0)
    compact_col = lax.broadcasted_iota(jnp.int32, (rows, per * 8), 1)
    third = (compact_row * 11) >> 5
    meets = ((compact_col >> 3) == third) & ((compact_col & 3) == compact_row - 3 * third)
    first = jnp.where(meets & ((compact_col & 4) == 0), 1.0, 0.0)
    second = jnp.where(meets & ((compact_col & 4) == 4), 1.0, 0.0)
    first_c, second_c = first.astype(BF16), second.astype(BF16)
    first_e, second_e = first.T.astype(BF16), second.T.astype(BF16)

    summed = []
    for sender in range(2):
        here, weight, _ = placed(1 - sender)
        summed.append(here * weight)
    exact = jnp.concatenate(summed, axis=0).T
    lane_half = (lax.broadcasted_iota(jnp.int32, exact.shape, 1) >> 2) & 1
    mixing = []
    for part in range(2):
        kept = jnp.where(lane_half == part, exact, 0.0)
        high = kept.astype(BF16)
        mixing += [high, (kept - high.astype(F32)).astype(BF16)]
    mixing = jnp.concatenate(mixing, axis=0)

    far_rows, near_rows = (1, 2), (0,)
    groups = (far_rows, near_rows)
    spans = [pl.ds(g[0] * rows, len(g) * rows) for g in groups]
    for k in (2, 1, 0):
        part = rbuf.at[pl.ds(k * per, per)]
        remote(part, part, d_send, d_recv.at[k], partner).wait_recv()
        got = part[...].astype(F32).reshape(per * 8, half).astype(BF16)
        span = pl.ds(k * rows, rows)
        xs[0, span, :half] = dot(first_c, got).astype(BF16)
        xs[0, span, half:] = dot(second_c, got).astype(BF16)
        g = 0 if k in far_rows else 1
        whole = xs.at[0, span]
        left, right = xs.at[0, span, pl.ds(0, half)], xs.at[0, span, pl.ds(half, half)]
        remote(left, xs.at[3, span, pl.ds(0, half)], y_send, y_recv.at[2, g], dev(0, 0, 2, core)).start()
        remote(right, xs.at[3, span, pl.ds(half, half)], y_send, y_recv.at[2, g], dev(0, 0, -2, core)).start()
        remote(whole, xs.at[1, span], y_send, y_recv.at[0, g], dev(0, 0, 1, core)).start()
        remote(whole, xs.at[2, span], y_send, y_recv.at[1, g], dev(0, 0, -1, core)).start()

    for push in pushes:
        push.wait_recv()

    def hidden_of(g):
        sums = None
        for n, dy in enumerate((0, -1, 1, 2)):
            if n:
                part = xs.at[n, spans[g]]
                remote(part, part, y_send, y_recv.at[n - 1, g], partner).wait_recv()
            block = xs[n, spans[g]]
            span = pl.ds(pl.multiple_of(lax.rem(y + dy + SHARES, SHARES) * share, 128), share)
            terms = [
                lax.dot_general(block, w[side, :, span], (((1,), (1,)), ((), ())), preferred_element_type=F32)
                for side in range(2)
                for w in (gw, uw)
            ]
            sums = terms if sums is None else [a + b for a, b in zip(sums, terms)]
        hidden = []
        for side in range(2):
            gated = jnp.minimum(sums[2 * side], CLAMP_LIMIT)
            upper = jnp.clip(sums[2 * side + 1], -CLAMP_LIMIT, CLAMP_LIMIT)
            hidden.append(((upper + 1.0) * gated * jax.nn.sigmoid(SIGMOID_SCALE * gated)).astype(BF16))
        return hidden

    sign = 1 - 2 * core
    ahead, ahead2 = dev(0, 0, sign, core), dev(0, 0, 2 * sign, core)
    behind, behind2 = dev(0, 0, -sign, core), dev(0, 0, -2 * sign, core)

    def term(hidden, steps):
        to = lax.rem(y + steps * sign + ny, ny)
        return dot(hidden[0], dw[0, to]) + dot(hidden[1], dw[1, to])

    def ship(slot, g, value, to):
        ssend[slot, spans[g]] = value.astype(BF16)
        remote(
            ssend.at[slot, spans[g]], srecv.at[slot, spans[g]], s_send, s_recv.at[slot, g], to
        ).start()

    def take(slot, g):
        part = srecv.at[slot, spans[g]]
        remote(part, part, s_send, s_recv.at[slot, g], partner).wait_recv()
        return part[...].astype(F32)

    def first_stage(g, hidden):
        terms = {steps: term(hidden, steps) for steps in (4, 3, -3)}
        ship(0, g, terms[4], ahead2)
        ship(1, g, terms[3], ahead)
        ship(2, g, terms[-3], behind)
        terms = {steps: term(hidden, steps) for steps in (1, -1, 2, -2, 0)}
        ship(3, g, terms[1], ahead)
        ship(4, g, terms[-1], behind)
        own[0, spans[g]] = terms[2]
        own[1, spans[g]] = terms[-2]
        own[2, spans[g]] = terms[0]

    def relay(g):
        ship(5, g, own[0, spans[g]] + take(0, g) + take(1, g), ahead2)
        ship(6, g, own[1, spans[g]] + take(2, g), behind2)

    is_0 = core == 0
    lane = 128

    def give_back(g):
        total = own[2, spans[g]]
        for slot in (3, 4, 6, 5):
            total = total + take(slot, g)
        total = total.astype(BF16)
        for k in reversed(groups[g]):
            at = (k - groups[g][0]) * rows
            piece = total[at : at + rows]
            ends, middle = dot(first_e, piece), dot(second_e, piece[:, lane : 2 * lane])
            spread_0, spread_1 = ends[:, :lane] + middle, ends[:, 2 * lane :] + middle
            span = pl.ds(k * per, per)
            same = jnp.where(is_0, spread_0, spread_1).reshape(per, 8, lane).astype(BF16)
            cross = jnp.where(is_0, spread_1, spread_0).reshape(per, 8, lane).astype(BF16)
            rsend[0, span] = same
            rsend[1, span] = cross
            for j in reversed(range(k * per, (k + 1) * per)):
                remote(rsend.at[1, j], rret.at[core, j], r_send.at[1], r_recv.at[1, g], source(j, other)).start()
                if j:
                    remote(rsend.at[0, j], rret.at[core, j], r_send.at[0], r_recv.at[0, g], source(j, core)).start()
                    continue

                @pl.when(is_0)
                def _():
                    remote(rsend.at[0, 0], rret.at[core, 0], r_send.at[2], r_recv.at[0, 2], source(0, core)).start()

                @pl.when(core == 1)
                def _():
                    rret[1, 0] = same[0]

    first_stage(0, hidden_of(0))
    first_stage(1, hidden_of(1))
    relay(0)
    give_back(0)
    relay(1)
    give_back(1)

    for g in range(2):
        begin, count = groups[g][0] * per, len(groups[g]) * per
        crossed = rret.at[other, pl.ds(begin, count)]
        remote(crossed, crossed, d_send, r_recv.at[1, g], partner).wait_recv()
        skipped = 0 if begin else 1
        stayed = rret.at[core, pl.ds(begin + skipped, count - skipped)]
        remote(stayed, stayed, d_send, r_recv.at[0, g], partner).wait_recv()

    own_chip = remote(rsend.at[0, 0], rret.at[core, 0], r_send.at[2], r_recv.at[0, 2], partner)

    @pl.when(is_0)
    def _():
        own_chip.wait_recv()

    back = rret[...].astype(F32).reshape(2 * peers * 8, lane).astype(BF16)
    mixed = dot(mixing, back)
    ends = mixed[:toks] + mixed[toks : 2 * toks]
    middle = mixed[2 * toks : 3 * toks] + mixed[3 * toks :]
    out_0 = jnp.concatenate([ends, middle[:, : lanes - lane]], axis=1)
    out_1 = jnp.concatenate([middle[:, 2 * lane - lanes :], ends], axis=1)
    out_ref[...] = jnp.where(is_0, out_0, out_1).astype(BF16)

    remote(sbuf, rbuf, d_send, d_recv.at[0], partner).wait_send()
    for push in pushes:
        push.wait_send()
    others = xs.at[pl.ds(1, 3)]
    remote(others, others, y_send, d_recv.at[0], partner).wait_send()
    remote(ssend, srecv, s_send, d_recv.at[0], partner).wait_send()
    remote(rsend.at[1], rret.at[0], r_send.at[1], d_recv.at[0], partner).wait_send()
    stayed = rsend.at[0, pl.ds(1, peers - 1)]
    remote(stayed, stayed, r_send.at[0], d_recv.at[0], partner).wait_send()

    @pl.when(is_0)
    def _():
        own_chip.wait_send()


def local(nz, ny, tokens, norm_gain, routing, route_weight, w_gate, w_up, w_down):
    toks, width = tokens.shape
    depth = w_gate.shape[2]
    peers = nz * NX // 2
    per = peers // CHUNKS
    rows = per * 3
    share = width // SHARES
    half = share // 2
    out_width = width // ny
    vmem = functools.partial(pl.BlockSpec, memory_space=pltpu.VMEM)
    hbm = functools.partial(pl.BlockSpec, memory_space=pl.ANY)
    dma = pltpu.SemaphoreType.DMA
    return pl.pallas_call(
        functools.partial(kernel, nz, ny),
        out_shape=jax.ShapeDtypeStruct((toks, width // (2 * ny)), BF16),
        in_specs=[hbm()] * 7,
        out_specs=vmem(),
        scratch_shapes=[
            pltpu.VMEM((toks, width), BF16),
            pltpu.VMEM((1, width), F32),
            pltpu.VMEM(routing.shape[::-1], jnp.int32),
            pltpu.VMEM(routing.shape[::-1], F32),
            pltpu.VMEM((2, depth, width), BF16),
            pltpu.VMEM((2, depth, width), BF16),
            pltpu.VMEM((2, ny, depth, out_width), BF16),
            pltpu.VMEM((peers, 8, half), BF16),
            pltpu.VMEM((peers, 8, half), BF16),
            pltpu.VMEM((SHARES, CHUNKS * rows, share), BF16),
            pltpu.VMEM((3, CHUNKS * rows, out_width), F32),
            pltpu.VMEM((ny - 1, CHUNKS * rows, out_width), BF16),
            pltpu.VMEM((ny - 1, CHUNKS * rows, out_width), BF16),
            pltpu.VMEM((2, peers, 8, 128), BF16),
            pltpu.VMEM((2, peers, 8, 128), BF16),
            dma((4,)),
            dma((3,)),
            dma((3,)),
            dma((3,)),
            dma,
            dma((CHUNKS,)),
            dma,
            dma((3, 2)),
            dma,
            dma((ny - 1, 2)),
            dma((3,)),
            dma((2, 3)),
        ],
        compiler_params=pltpu.CompilerParams(collective_id=0, has_side_effects=True),
    )(
        tokens,
        norm_gain.reshape(1, width),
        routing.T,
        route_weight.T,
        w_gate[0].T,
        w_up[0].T,
        w_down.reshape(depth, width),
    )


def solution(mesh):
    placed = (
        P("ep", None),
        P(),
        P("ep", None),
        P("ep", None),
        P("ep", None, "tp"),
        P("ep", None, "tp"),
        P("ep", "tp", None),
    )
    body = functools.partial(local, mesh.shape["ep"] // NX, mesh.shape["tp"] // 2)
    return jax.shard_map(body, mesh=mesh, in_specs=placed, out_specs=P("ep", "tp"), check_vma=False)
```

```python
import functools

import jax
import jax.numpy as jnp
from jax import lax
from jax.experimental import pallas as pl
from jax.experimental.pallas import tpu as pltpu
from jax.sharding import PartitionSpec as P

NORM_EPS = 1e-06
CLAMP_LIMIT = 7.0
SIGMOID_SCALE = 1.702
MESH = pl.DeviceIdType.MESH
NX = 4
CHUNKS = 3
SHARES = 4
F32 = jnp.float32
BF16 = jnp.bfloat16


def dot(a, b):
    return jnp.dot(a, b, preferred_element_type=F32)


def kernel(
    nz, ny, tok_hbm, gain_hbm, route_hbm, rw_hbm, wg_ref, wu_ref, wd_ref, out_ref,
    tok_ref, gain_ref, route_ref, rw_ref, gw, uw, dw, sbuf, rbuf, xs, acc, own, ssend, srecv, rsend, rret,
    in_sem, w_sem, wp_send, wp_recv, d_send, d_recv, y_send, y_recv, s_send, s_recv, r_send, r_recv,
):
    ep, tp = lax.axis_index("ep"), lax.axis_index("tp")
    z, x = lax.div(ep, NX), lax.rem(ep, NX)
    y, core = lax.div(tp, 2), lax.rem(tp, 2)
    other = 1 - core
    toks = tok_ref.shape[0]
    peers = sbuf.shape[0]
    per = peers // CHUNKS
    half = sbuf.shape[2]
    share = 2 * half
    lanes = out_ref.shape[1]

    def dev(dz, dx, dy, at):
        return (
            lax.rem(z + dz + 2 * nz, nz) * NX + lax.rem(x + dx + NX, NX),
            lax.rem(y + dy + ny, ny) * 2 + at,
        )

    def offset(j, sender):
        return nz // 4 + sender * (nz // 2) + j // NX, (j + 1) % NX

    def remote(src, dst, send, recv, to):
        return pltpu.make_async_remote_copy(
            src_ref=src, dst_ref=dst, send_sem=send, recv_sem=recv, device_id=to, device_id_type=MESH
        )

    partner = dev(0, 0, 0, other)
    def source(j, at):
        dz, dx = offset(j, other)
        return dev(-dz, -dx, 0, at)

    sources = [source(j, other) for j in range(peers)]
    targets = [dev(*offset(j, core), 0, other) for j in range(peers)]
    own_slot = peers // 2 + NX - 1
    chunk_order = (1, 2, 0)

    barrier = pltpu.get_barrier_semaphore()
    for to in sources + [dev(0, 0, dy, core) for dy in (2, -2, 1, -1)] + [partner]:
        pl.semaphore_signal(barrier, inc=1, device_id=to, device_id_type=MESH)

    fetches = [
        pltpu.make_async_copy(src, dst, in_sem.at[n])
        for n, (src, dst) in enumerate(
            ((tok_hbm, tok_ref), (gain_hbm, gain_ref), (route_hbm, route_ref), (rw_hbm, rw_ref))
        )
    ]
    for fetch in fetches:
        fetch.start()
    local = [
        pltpu.make_async_copy(wg_ref, gw.at[0], w_sem.at[0]),
        pltpu.make_async_copy(wu_ref, uw.at[0], w_sem.at[1]),
    ]
    for copy in local:
        copy.start()
    out_width = dw.shape[3]
    for q in range(ny):
        pltpu.make_async_copy(
            wd_ref.at[:, pl.ds(q * out_width, out_width)], dw.at[0, q], w_sem.at[2]
        ).start()

    for fetch in fetches:
        fetch.wait()
    values = tok_ref[...].astype(F32)
    scale = lax.rsqrt(jnp.mean(values * values, axis=-1, keepdims=True) + NORM_EPS)
    at = pl.multiple_of(lax.rem(y, SHARES) * share, 128)
    shared = tok_ref[:, pl.ds(at, share)].astype(F32)
    normal = (shared * scale * gain_ref[:, pl.ds(at, share)]).astype(BF16)

    routes, weights = route_ref[...], rw_ref[...]
    earlier = jnp.where(
        lax.broadcasted_iota(jnp.int32, (toks, toks), 0) < lax.broadcasted_iota(jnp.int32, (toks, toks), 1),
        1.0,
        0.0,
    ).astype(BF16)

    def placed(sender):
        row = lax.broadcasted_iota(jnp.int32, (peers * 8, 1), 0)
        ez = z + nz // 4 + sender * (nz // 2) + (row >> 5)
        ez = jnp.where(ez >= nz, ez - nz, ez)
        ez = jnp.where(ez >= nz, ez - nz, ez)
        expert = ez * NX + ((x + (row >> 3) + 1) & (NX - 1))
        hit = jnp.zeros((peers * 8, toks), F32)
        weight = jnp.zeros((peers * 8, toks), F32)
        for k in range(routes.shape[0]):
            same = routes[k : k + 1] == expert
            hit = hit + jnp.where(same, 1.0, 0.0)
            weight = weight + jnp.where(same, weights[k : k + 1], 0.0)
        before = dot(hit.astype(BF16), earlier)
        here = jnp.where(before == (row & 3).astype(F32), hit, 0.0)
        return here, weight, (row >> 2) & 1

    here, _, in_half = placed(core)
    here_0 = jnp.where(in_half == 0, here, 0.0)
    here_1 = here - here_0
    sending = dot(here_0.astype(BF16), normal[:, :half]) + dot(here_1.astype(BF16), normal[:, half:])
    sbuf[...] = sending.reshape(peers, 8, half).astype(BF16)

    pl.semaphore_wait(barrier, peers + 5)
    for j in [k * per + n for k in chunk_order for n in range(per)]:
        remote(sbuf.at[j], rbuf.at[j], d_send, d_recv.at[j // per], targets[j]).start()

    for copy in local:
        copy.wait()
    pltpu.make_async_copy(dw.at[0], dw.at[0], w_sem.at[2]).wait()
    pushes = [
        remote(buf.at[0], buf.at[1], wp_send.at[n], wp_recv.at[n], partner)
        for n, buf in enumerate((gw, uw, dw))
    ]
    for push in pushes:
        push.start()

    rows = per * 3
    compact_row = lax.broadcasted_iota(jnp.int32, (rows, per * 8), 0)
    compact_col = lax.broadcasted_iota(jnp.int32, (rows, per * 8), 1)
    third = (compact_row * 11) >> 5
    meets = ((compact_col >> 3) == third) & ((compact_col & 3) == compact_row - 3 * third)
    first = jnp.where(meets & ((compact_col & 4) == 0), 1.0, 0.0)
    second = jnp.where(meets & ((compact_col & 4) == 4), 1.0, 0.0)
    first_c, second_c = first.astype(BF16), second.astype(BF16)
    first_e, second_e = first.T.astype(BF16), second.T.astype(BF16)

    summed = []
    for sender in range(2):
        here, weight, _ = placed(1 - sender)
        summed.append(here * weight)
    exact = jnp.concatenate(summed, axis=0).T
    lane_half = (lax.broadcasted_iota(jnp.int32, exact.shape, 1) >> 2) & 1
    mixing = []
    for part in range(2):
        kept = jnp.where(lane_half == part, exact, 0.0)
        high = kept.astype(BF16)
        mixing += [high, (kept - high.astype(F32)).astype(BF16)]
    mixing = jnp.concatenate(mixing, axis=0)

    spans = [pl.ds(k * rows, rows) for k in chunk_order]
    for g, k in enumerate(chunk_order):
        part = rbuf.at[pl.ds(k * per, per)]
        remote(part, part, d_send, d_recv.at[k], partner).wait_recv()
        got = part[...].astype(F32).reshape(per * 8, half).astype(BF16)
        span = pl.ds(k * rows, rows)
        xs[0, span, :half] = dot(first_c, got).astype(BF16)
        xs[0, span, half:] = dot(second_c, got).astype(BF16)
        whole = xs.at[0, span]
        left, right = xs.at[0, span, pl.ds(0, half)], xs.at[0, span, pl.ds(half, half)]
        remote(left, xs.at[3, span, pl.ds(0, half)], y_send, y_recv.at[2, g], dev(0, 0, 2, core)).start()
        remote(right, xs.at[3, span, pl.ds(half, half)], y_send, y_recv.at[2, g], dev(0, 0, -2, core)).start()
        remote(whole, xs.at[1, span], y_send, y_recv.at[0, g], dev(0, 0, 1, core)).start()
        remote(whole, xs.at[2, span], y_send, y_recv.at[1, g], dev(0, 0, -1, core)).start()

    for push in pushes:
        push.wait_recv()

    def products(block, dy):
        span = pl.ds(pl.multiple_of(lax.rem(y + dy + SHARES, SHARES) * share, 128), share)
        return [
            lax.dot_general(block, w[side, :, span], (((1,), (1,)), ((), ())), preferred_element_type=F32)
            for side in range(2)
            for w in (gw, uw)
        ]

    for n, product in enumerate(products(xs[0], 0)):
        acc[n] = product

    def hidden_of(g):
        sums = [acc[n, spans[g]] for n in range(4)]
        for n, dy in ((1, -1), (2, 1), (3, 2)):
            part = xs.at[n, spans[g]]
            remote(part, part, y_send, y_recv.at[n - 1, g], partner).wait_recv()
            sums = [a + b for a, b in zip(sums, products(part[...], dy))]
        hidden = []
        for side in range(2):
            gated = jnp.minimum(sums[2 * side], CLAMP_LIMIT)
            upper = jnp.clip(sums[2 * side + 1], -CLAMP_LIMIT, CLAMP_LIMIT)
            hidden.append(((upper + 1.0) * gated * jax.nn.sigmoid(SIGMOID_SCALE * gated)).astype(BF16))
        return hidden

    sign = 1 - 2 * core
    ahead, ahead2 = dev(0, 0, sign, core), dev(0, 0, 2 * sign, core)
    behind, behind2 = dev(0, 0, -sign, core), dev(0, 0, -2 * sign, core)

    def term(hidden, steps):
        to = lax.rem(y + steps * sign + ny, ny)
        return dot(hidden[0], dw[0, to]) + dot(hidden[1], dw[1, to])

    def ship(slot, g, value, to):
        ssend[slot, spans[g]] = value.astype(BF16)
        remote(
            ssend.at[slot, spans[g]], srecv.at[slot, spans[g]], s_send, s_recv.at[slot, g], to
        ).start()

    def take(slot, g):
        part = srecv.at[slot, spans[g]]
        remote(part, part, s_send, s_recv.at[slot, g], partner).wait_recv()
        return part[...].astype(F32)

    def first_stage(g, hidden):
        terms = {steps: term(hidden, steps) for steps in (4, 3, -3)}
        ship(0, g, terms[4], ahead2)
        ship(1, g, terms[3], ahead)
        ship(2, g, terms[-3], behind)
        terms = {steps: term(hidden, steps) for steps in (1, -1, 2, -2, 0)}
        ship(3, g, terms[1], ahead)
        ship(4, g, terms[-1], behind)
        own[0, spans[g]] = terms[2]
        own[1, spans[g]] = terms[-2]
        own[2, spans[g]] = terms[0]

    def relay(g):
        ship(5, g, own[0, spans[g]] + take(0, g) + take(1, g), ahead2)
        ship(6, g, own[1, spans[g]] + take(2, g), behind2)

    is_0 = core == 0
    lane = 128
    own_chip = remote(
        rsend.at[0, own_slot], rret.at[core, own_slot], r_send.at[3], r_recv.at[0, CHUNKS], source(own_slot, core)
    )

    def give_back(g):
        total = own[2, spans[g]]
        for slot in (3, 4, 6, 5):
            total = total + take(slot, g)
        total = total.astype(BF16)
        ends, middle = dot(first_e, total), dot(second_e, total[:, lane : 2 * lane])
        spread_0, spread_1 = ends[:, :lane] + middle, ends[:, 2 * lane :] + middle
        first_slot = chunk_order[g] * per
        span = pl.ds(first_slot, per)
        same = jnp.where(is_0, spread_0, spread_1).reshape(per, 8, lane).astype(BF16)
        cross = jnp.where(is_0, spread_1, spread_0).reshape(per, 8, lane).astype(BF16)
        rsend[0, span] = same
        rsend[1, span] = cross
        for j in range(first_slot, first_slot + per):
            remote(rsend.at[1, j], rret.at[core, j], r_send.at[1], r_recv.at[1, g], source(j, other)).start()
            if j != own_slot:
                to, half_send = source(j, core), r_send.at[0 if j < own_slot else 2]
                remote(rsend.at[0, j], rret.at[core, j], half_send, r_recv.at[0, g], to).start()
                continue

            @pl.when(core == 1)
            def _():
                own_chip.start()

            @pl.when(is_0)
            def _():
                rret[0, own_slot] = same[own_slot - first_slot]

    for g in range(CHUNKS):
        first_stage(g, hidden_of(g))
    for g in range(CHUNKS):
        relay(g)
    for g in range(CHUNKS):
        give_back(g)

    for g, k in enumerate(chunk_order):
        crossed = rret.at[other, pl.ds(k * per, per)]
        remote(crossed, crossed, d_send, r_recv.at[1, g], partner).wait_recv()
        count = per - 1 if own_slot // per == k else per
        stayed = rret.at[core, pl.ds(k * per, count)]
        remote(stayed, stayed, d_send, r_recv.at[0, g], partner).wait_recv()

    @pl.when(core == 1)
    def _():
        own_chip.wait_recv()

    back = rret[...].astype(F32).reshape(2 * peers * 8, lane).astype(BF16)
    mixed = dot(mixing, back)
    ends = mixed[:toks] + mixed[toks : 2 * toks]
    middle = mixed[2 * toks : 3 * toks] + mixed[3 * toks :]
    out_0 = jnp.concatenate([ends, middle[:, : lanes - lane]], axis=1)
    out_1 = jnp.concatenate([middle[:, 2 * lane - lanes :], ends], axis=1)
    out_ref[...] = jnp.where(is_0, out_0, out_1).astype(BF16)

    remote(sbuf, rbuf, d_send, d_recv.at[0], partner).wait_send()
    for push in pushes:
        push.wait_send()
    others = xs.at[pl.ds(1, 3)]
    remote(others, others, y_send, d_recv.at[0], partner).wait_send()
    remote(ssend, srecv, s_send, d_recv.at[0], partner).wait_send()
    remote(rsend.at[1], rret.at[0], r_send.at[1], d_recv.at[0], partner).wait_send()
    for n, begin, count in ((0, 0, own_slot), (2, own_slot + 1, peers - 1 - own_slot)):
        stayed = rsend.at[0, pl.ds(begin, count)]
        remote(stayed, stayed, r_send.at[n], d_recv.at[0], partner).wait_send()

    @pl.when(core == 1)
    def _():
        own_chip.wait_send()


def local(nz, ny, tokens, norm_gain, routing, route_weight, w_gate, w_up, w_down):
    toks, width = tokens.shape
    depth = w_gate.shape[2]
    peers = nz * NX // 2
    per = peers // CHUNKS
    rows = per * 3
    share = width // SHARES
    half = share // 2
    out_width = width // ny
    vmem = functools.partial(pl.BlockSpec, memory_space=pltpu.VMEM)
    hbm = functools.partial(pl.BlockSpec, memory_space=pl.ANY)
    dma = pltpu.SemaphoreType.DMA
    return pl.pallas_call(
        functools.partial(kernel, nz, ny),
        out_shape=jax.ShapeDtypeStruct((toks, width // (2 * ny)), BF16),
        in_specs=[hbm()] * 7,
        out_specs=vmem(),
        scratch_shapes=[
            pltpu.VMEM((toks, width), BF16),
            pltpu.VMEM((1, width), F32),
            pltpu.VMEM(routing.shape[::-1], jnp.int32),
            pltpu.VMEM(routing.shape[::-1], F32),
            pltpu.VMEM((2, depth, width), BF16),
            pltpu.VMEM((2, depth, width), BF16),
            pltpu.VMEM((2, ny, depth, out_width), BF16),
            pltpu.VMEM((peers, 8, half), BF16),
            pltpu.VMEM((peers, 8, half), BF16),
            pltpu.VMEM((SHARES, CHUNKS * rows, share), BF16),
            pltpu.VMEM((4, CHUNKS * rows, depth), F32),
            pltpu.VMEM((3, CHUNKS * rows, out_width), F32),
            pltpu.VMEM((ny - 1, CHUNKS * rows, out_width), BF16),
            pltpu.VMEM((ny - 1, CHUNKS * rows, out_width), BF16),
            pltpu.VMEM((2, peers, 8, 128), BF16),
            pltpu.VMEM((2, peers, 8, 128), BF16),
            dma((4,)),
            dma((3,)),
            dma((3,)),
            dma((3,)),
            dma,
            dma((CHUNKS,)),
            dma,
            dma((3, CHUNKS)),
            dma,
            dma((ny - 1, CHUNKS)),
            dma((4,)),
            dma((2, CHUNKS + 1)),
        ],
        compiler_params=pltpu.CompilerParams(collective_id=0, has_side_effects=True),
    )(
        tokens,
        norm_gain.reshape(1, width),
        routing.T,
        route_weight.T,
        w_gate[0].T,
        w_up[0].T,
        w_down.reshape(depth, width),
    )


def solution(mesh):
    placed = (
        P("ep", None),
        P(),
        P("ep", None),
        P("ep", None),
        P("ep", None, "tp"),
        P("ep", None, "tp"),
        P("ep", "tp", None),
    )
    body = functools.partial(local, mesh.shape["ep"] // NX, mesh.shape["tp"] // 2)
    return jax.shard_map(body, mesh=mesh, in_specs=placed, out_specs=P("ep", "tp"), check_vma=False)
```

```python
import functools

import jax
import jax.numpy as jnp
from jax import lax
from jax.experimental import pallas as pl
from jax.experimental.pallas import tpu as pltpu
from jax.sharding import PartitionSpec as P

NORM_EPS = 1e-06
CLAMP_LIMIT = 7.0
SIGMOID_SCALE = 1.702
MESH = pl.DeviceIdType.MESH
NX = 4
CHUNKS = 3
SHARES = 4
F32 = jnp.float32
BF16 = jnp.bfloat16


def dot(a, b):
    return jnp.dot(a, b, preferred_element_type=F32)


def kernel(
    nz, ny, tok_hbm, gain_hbm, route_hbm, rw_hbm, wg_ref, wu_ref, wd_ref, out_ref,
    tok_ref, gain_ref, route_ref, rw_ref, guw, dw, packed, spilled, gathered, sbuf, rbuf, xs, acc, own, ssend, srecv, rsend, rret,
    in_sem, w_sem, wp_send, wp_recv, d_send, d_recv, y_send, y_recv, s_send, s_recv, r_send, r_recv,
):
    ep, tp = lax.axis_index("ep"), lax.axis_index("tp")
    z, x = lax.div(ep, NX), lax.rem(ep, NX)
    y, core = lax.div(tp, 2), lax.rem(tp, 2)
    other = 1 - core
    toks, depth = tok_ref.shape[0], wd_ref.shape[0]
    peers = sbuf.shape[0]
    per = peers // CHUNKS
    half = xs.shape[2] // 2
    share = 2 * half
    lanes = out_ref.shape[1]

    def dev(dz, dx, dy, at):
        return (
            lax.rem(z + dz + 2 * nz, nz) * NX + lax.rem(x + dx + NX, NX),
            lax.rem(y + dy + ny, ny) * 2 + at,
        )

    def offset(j, sender):
        return nz // 4 + sender * (nz // 2) + j // NX, (j + 1) % NX

    def remote(src, dst, send, recv, to):
        return pltpu.make_async_remote_copy(
            src_ref=src, dst_ref=dst, send_sem=send, recv_sem=recv, device_id=to, device_id_type=MESH
        )

    partner = dev(0, 0, 0, other)
    def source(j, at):
        dz, dx = offset(j, other)
        return dev(-dz, -dx, 0, at)

    sources = [source(j, other) for j in range(peers)]
    targets = [dev(*offset(j, core), 0, other) for j in range(peers)]
    own_slot = peers // 2 + NX - 1
    chunk_order = (1, 2, 0)

    barrier = pltpu.get_barrier_semaphore()
    for to in sources + [dev(0, 0, dy, core) for dy in (2, -2, 1, -1)] + [partner]:
        pl.semaphore_signal(barrier, inc=1, device_id=to, device_id_type=MESH)

    fetches = [
        pltpu.make_async_copy(src, dst, in_sem.at[n])
        for n, (src, dst) in enumerate(
            ((tok_hbm, tok_ref), (gain_hbm, gain_ref), (route_hbm, route_ref), (rw_hbm, rw_ref))
        )
    ]
    for fetch in fetches:
        fetch.start()
    local = [
        pltpu.make_async_copy(wg_ref, guw.at[0], w_sem.at[0]),
        pltpu.make_async_copy(wu_ref, guw.at[2], w_sem.at[1]),
    ]
    for copy in local:
        copy.start()
    out_width = dw.shape[3]
    for q in range(ny):
        pltpu.make_async_copy(
            wd_ref.at[:, pl.ds(q * out_width, out_width)], dw.at[0, q], w_sem.at[2]
        ).start()

    for fetch in fetches:
        fetch.wait()
    values = tok_ref[...].astype(F32)
    scale = lax.rsqrt(jnp.mean(values * values, axis=-1, keepdims=True) + NORM_EPS)
    at = pl.multiple_of(lax.rem(y, SHARES) * share, 128)
    shared = tok_ref[:, pl.ds(at, share)].astype(F32)
    normal = (shared * scale * gain_ref[:, pl.ds(at, share)]).astype(BF16)

    routes, weights = route_ref[...], rw_ref[...]
    earlier = jnp.where(
        lax.broadcasted_iota(jnp.int32, (toks, toks), 0) < lax.broadcasted_iota(jnp.int32, (toks, toks), 1),
        1.0,
        0.0,
    ).astype(BF16)

    def named(sender, peer):
        ez = z + nz // 4 + sender * (nz // 2) + (peer >> 2)
        ez = jnp.where(ez >= nz, ez - nz, ez)
        ez = jnp.where(ez >= nz, ez - nz, ez)
        expert = ez * NX + ((x + peer + 1) & (NX - 1))
        hit = jnp.zeros((peer.shape[0], toks), F32)
        weight = jnp.zeros((peer.shape[0], toks), F32)
        for k in range(routes.shape[0]):
            same = routes[k : k + 1] == expert
            hit = hit + jnp.where(same, 1.0, 0.0)
            weight = weight + jnp.where(same, weights[k : k + 1], 0.0)
        return hit, weight, dot(hit.astype(BF16), earlier)

    row = lax.broadcasted_iota(jnp.int32, (peers * 2, 1), 0)
    hit, _, before = named(core, row >> 1)

    def pick(at, place):
        return jnp.where(((row & 1) == at) & (before == place), hit, 0.0).astype(BF16)

    first_half, second_half = normal[:, :half], normal[:, half:]
    upper_0, upper_1, lower_1, lower_2 = pick(0, 0.0), pick(0, 1.0), pick(1, 1.0), pick(1, 2.0)
    packed[:, pl.ds(0, half)] = dot(upper_0, first_half) + dot(lower_1, second_half)
    packed[:, pl.ds(half, half)] = dot(upper_0, second_half) + dot(lower_2, first_half)
    packed[:, pl.ds(share, half)] = dot(upper_1, first_half) + dot(lower_2, second_half)
    for j in range(peers):
        sbuf[j] = packed[pl.ds(2 * j, 2)].astype(BF16)

    pl.semaphore_wait(barrier, peers + 5)
    for j in [k * per + n for k in chunk_order for n in range(per)]:
        remote(sbuf.at[j], rbuf.at[j], d_send, d_recv.at[j // per], targets[j]).start()

    for copy in local:
        copy.wait()
    pltpu.make_async_copy(dw.at[0], dw.at[0], w_sem.at[2]).wait()
    pushes = [
        remote(src, dst, wp_send.at[n], wp_recv.at[n], partner)
        for n, (src, dst) in enumerate(
            ((guw.at[0], guw.at[1]), (guw.at[2], guw.at[3]), (dw.at[0], dw.at[1]))
        )
    ]
    for push in pushes:
        push.start()

    rows = per * 3
    to_row = lax.broadcasted_iota(jnp.int32, (rows, per * 6), 0)
    from_row = lax.broadcasted_iota(jnp.int32, (rows, per * 6), 1)
    third, block = (to_row * 11) >> 5, from_row >> 4
    meets = (((from_row & 15) >> 1) == third) & (block == to_row - 3 * third)
    first_c = jnp.where(meets & ((from_row & 1) == (block >> 1)), 1.0, 0.0).astype(BF16)
    second_c = jnp.where(meets & ((from_row & 1) == ((block + 1) >> 1)), 1.0, 0.0).astype(BF16)
    to_row = lax.broadcasted_iota(jnp.int32, (per * 6, rows), 0)
    from_row = lax.broadcasted_iota(jnp.int32, (per * 6, rows), 1)
    meets = from_row == 3 * ((to_row & 15) >> 1) + (to_row >> 4)
    first_e = jnp.where(meets & ((to_row & 1) == 0), 1.0, 0.0).astype(BF16)
    second_e = jnp.where(meets & ((to_row & 1) == 1), 1.0, 0.0).astype(BF16)

    row = lax.broadcasted_iota(jnp.int32, (peers * 12, 1), 0)
    place = jnp.where(row >= peers * 4, 1, 0) + jnp.where(row >= peers * 8, 1, 0)
    row = row - place * (peers * 4)
    holder = jnp.where(row >= peers * 2, 1, 0)
    hit, weight, before = named(1 - holder, (row - holder * (peers * 2)) >> 1)
    exact = jnp.where(before == place.astype(F32), hit * weight, 0.0).T
    lane_part = lax.broadcasted_iota(jnp.int32, exact.shape, 1) & 1
    mixing = []
    for part in range(2):
        kept = jnp.where(lane_part == part, exact, 0.0)
        high = kept.astype(BF16)
        mixing += [high, (kept - high.astype(F32)).astype(BF16)]
    mixing = jnp.concatenate(mixing, axis=0)

    spans = [pl.ds(g * rows, rows) for g in range(CHUNKS)]
    for g, k in enumerate(chunk_order):
        part = rbuf.at[pl.ds(k * per, per)]
        remote(part, part, d_send, d_recv.at[k], partner).wait_recv()
        for n in range(per):
            packed[pl.ds(2 * n, 2)] = rbuf[k * per + n].astype(F32)
        blocks = [packed[pl.ds(0, 2 * per), pl.ds(n * half, half)].astype(BF16) for n in range(3)]
        span = spans[g]
        xs[0, span, :half] = dot(first_c, jnp.concatenate([blocks[0], blocks[2], blocks[1]], axis=0)).astype(BF16)
        xs[0, span, half:] = dot(second_c, jnp.concatenate([blocks[1], blocks[0], blocks[2]], axis=0)).astype(BF16)
        whole = xs.at[0, span]
        left, right = xs.at[0, span, pl.ds(0, half)], xs.at[0, span, pl.ds(half, half)]
        remote(left, xs.at[3, span, pl.ds(0, half)], y_send, y_recv.at[2, g], dev(0, 0, 2, core)).start()
        remote(right, xs.at[3, span, pl.ds(half, half)], y_send, y_recv.at[2, g], dev(0, 0, -2, core)).start()
        remote(whole, xs.at[1, span], y_send, y_recv.at[0, g], dev(0, 0, 1, core)).start()
        remote(whole, xs.at[2, span], y_send, y_recv.at[1, g], dev(0, 0, -1, core)).start()

    for push in pushes:
        push.wait_recv()

    def products(block, dy):
        span = pl.ds(pl.multiple_of(lax.rem(y + dy + SHARES, SHARES) * share, 128), share)
        both = guw[:, :, span].reshape(4 * depth, share)
        return lax.dot_general(block, both, (((1,), (1,)), ((), ())), preferred_element_type=F32)

    acc[...] = products(xs[0], 0)

    def hidden_of(gs):
        span = pl.ds(gs[0] * rows, len(gs) * rows)
        sums = acc[span]
        for n, dy in ((1, -1), (2, 1), (3, 2)):
            for g in gs:
                part = xs.at[n, spans[g]]
                remote(part, part, y_send, y_recv.at[n - 1, g], partner).wait_recv()
            sums = sums + products(xs[n, span], dy)
        gated = jnp.minimum(sums[:, : 2 * depth], CLAMP_LIMIT)
        upper = jnp.clip(sums[:, 2 * depth :], -CLAMP_LIMIT, CLAMP_LIMIT)
        return ((upper + 1.0) * gated * jax.nn.sigmoid(SIGMOID_SCALE * gated)).astype(BF16)

    sign = 1 - 2 * core
    ahead, ahead2 = dev(0, 0, sign, core), dev(0, 0, 2 * sign, core)
    behind, behind2 = dev(0, 0, -sign, core), dev(0, 0, -2 * sign, core)

    def terms(hidden, steps):
        blocks = []
        for step in steps:
            to = lax.rem(y + step * sign + ny, ny)
            blocks.append(jnp.concatenate([dw[0, to], dw[1, to]], axis=0))
        out = dot(hidden, jnp.concatenate(blocks, axis=1))
        return [out[:, n * out_width : (n + 1) * out_width] for n in range(len(steps))]

    def ship(slot, g, value, to):
        ssend[slot, spans[g]] = value.astype(BF16)
        launch(slot, g, to)

    def launch(slot, g, to):
        remote(
            ssend.at[slot, spans[g]], srecv.at[slot, spans[g]], s_send, s_recv.at[slot, g], to
        ).start()

    def take(slot, g):
        part = srecv.at[slot, spans[g]]
        remote(part, part, s_send, s_recv.at[slot, g], partner).wait_recv()
        return part[...].astype(F32)

    def first_stage(gs, hidden):
        to_ship = ((0, 4, ahead2), (1, 3, ahead), (2, -3, behind))
        out = terms(hidden, [step for _, step, _ in to_ship] + [2])
        for n, g in enumerate(gs):
            for (slot, _, to), value in zip(to_ship, out):
                ship(slot, g, value[n * rows : (n + 1) * rows], to)
            own[0, spans[g]] = out[3][n * rows : (n + 1) * rows]
        out = terms(hidden, (-2, 0, 1, -1))
        for n, g in enumerate(gs):
            for slot, value in enumerate(out[:2]):
                own[slot + 1, spans[g]] = value[n * rows : (n + 1) * rows]
            for slot, value in enumerate(out[2:]):
                ssend[slot + 3, spans[g]] = value[n * rows : (n + 1) * rows].astype(BF16)

    def neighbours(g):
        launch(3, g, ahead)
        launch(4, g, behind)

    def relay(g):
        ship(5, g, own[0, spans[g]] + take(0, g) + take(1, g), ahead2)
        ship(6, g, own[1, spans[g]] + take(2, g), behind2)

    is_0 = core == 0
    lane = 128
    own_chip = remote(
        rsend.at[0, own_slot], rret.at[core, own_slot], r_send.at[3], r_recv.at[0, CHUNKS], source(own_slot, core)
    )

    def give_back(g):
        total = own[2, spans[g]]
        for slot in (3, 4, 6, 5):
            total = total + take(slot, g)
        total = total.astype(BF16)
        ends, middle = dot(first_e, total), dot(second_e, total[:, lane : 2 * lane])
        first_slot = chunk_order[g] * per
        spreads = []
        for spread in (ends[:, :lane] + middle, ends[:, 2 * lane :] + middle):
            spreads.append(jnp.concatenate([spread[n * 2 * per : (n + 1) * 2 * per] for n in range(3)], axis=1))
        spilled[0] = jnp.where(is_0, spreads[0], spreads[1])
        spilled[1] = jnp.where(is_0, spreads[1], spreads[0])
        for n in range(per):
            rsend[0, first_slot + n] = spilled[0, pl.ds(2 * n, 2)].astype(BF16)
            rsend[1, first_slot + n] = spilled[1, pl.ds(2 * n, 2)].astype(BF16)
        for j in range(first_slot, first_slot + per):
            remote(rsend.at[1, j], rret.at[core, j], r_send.at[1], r_recv.at[1, g], source(j, other)).start()
            if j != own_slot:
                to, half_send = source(j, core), r_send.at[0 if j < own_slot else 2]
                remote(rsend.at[0, j], rret.at[core, j], half_send, r_recv.at[0, g], to).start()
                continue

            @pl.when(core == 1)
            def _():
                own_chip.start()

            @pl.when(is_0)
            def _():
                rret[0, own_slot] = rsend[0, own_slot]

    for gs in ((0,), (1, 2)):
        first_stage(gs, hidden_of(gs))
        if gs == (0,):
            neighbours(0)
    for g in range(CHUNKS):
        relay(g)
        if g + 1 < CHUNKS:
            neighbours(g + 1)
    for g in range(CHUNKS):
        give_back(g)

    for g, k in enumerate(chunk_order):
        crossed = rret.at[other, pl.ds(k * per, per)]
        remote(crossed, crossed, d_send, r_recv.at[1, g], partner).wait_recv()
        count = per - 1 if own_slot // per == k else per
        stayed = rret.at[core, pl.ds(k * per, count)]
        remote(stayed, stayed, d_send, r_recv.at[0, g], partner).wait_recv()

    @pl.when(core == 1)
    def _():
        own_chip.wait_recv()

    for holder in range(2):
        for j in range(peers):
            gathered[pl.ds((holder * peers + j) * 2, 2)] = rret[holder, j].astype(F32)
    back = gathered[...].astype(BF16)
    back = jnp.concatenate([back[:, n * lane : (n + 1) * lane] for n in range(3)], axis=0)
    mixed = dot(mixing, back)
    ends = mixed[:toks] + mixed[toks : 2 * toks]
    middle = mixed[2 * toks : 3 * toks] + mixed[3 * toks :]
    out_0 = jnp.concatenate([ends, middle[:, : lanes - lane]], axis=1)
    out_1 = jnp.concatenate([middle[:, 2 * lane - lanes :], ends], axis=1)
    out_ref[...] = jnp.where(is_0, out_0, out_1).astype(BF16)

    remote(sbuf, rbuf, d_send, d_recv.at[0], partner).wait_send()
    for push in pushes:
        push.wait_send()
    others = xs.at[pl.ds(1, 3)]
    remote(others, others, y_send, d_recv.at[0], partner).wait_send()
    remote(ssend, srecv, s_send, d_recv.at[0], partner).wait_send()
    remote(rsend.at[1], rret.at[0], r_send.at[1], d_recv.at[0], partner).wait_send()
    for n, begin, count in ((0, 0, own_slot), (2, own_slot + 1, peers - 1 - own_slot)):
        stayed = rsend.at[0, pl.ds(begin, count)]
        remote(stayed, stayed, r_send.at[n], d_recv.at[0], partner).wait_send()

    @pl.when(core == 1)
    def _():
        own_chip.wait_send()


def local(nz, ny, tokens, norm_gain, routing, route_weight, w_gate, w_up, w_down):
    toks, width = tokens.shape
    depth = w_gate.shape[2]
    peers = nz * NX // 2
    per = peers // CHUNKS
    rows = per * 3
    share = width // SHARES
    half = share // 2
    out_width = width // ny
    vmem = functools.partial(pl.BlockSpec, memory_space=pltpu.VMEM)
    hbm = functools.partial(pl.BlockSpec, memory_space=pl.ANY)
    dma = pltpu.SemaphoreType.DMA
    return pl.pallas_call(
        functools.partial(kernel, nz, ny),
        out_shape=jax.ShapeDtypeStruct((toks, width // (2 * ny)), BF16),
        in_specs=[hbm()] * 7,
        out_specs=vmem(),
        scratch_shapes=[
            pltpu.VMEM((toks, width), BF16),
            pltpu.VMEM((1, width), F32),
            pltpu.VMEM(routing.shape[::-1], jnp.int32),
            pltpu.VMEM(routing.shape[::-1], F32),
            pltpu.VMEM((4, depth, width), BF16),
            pltpu.VMEM((2, ny, depth, out_width), BF16),
            pltpu.VMEM((peers * 2, 3 * half), F32),
            pltpu.VMEM((2, per * 2, 384), F32),
            pltpu.VMEM((peers * 4, 384), F32),
            pltpu.VMEM((peers, 2, 3 * half), BF16),
            pltpu.VMEM((peers, 2, 3 * half), BF16),
            pltpu.VMEM((SHARES, CHUNKS * rows, share), BF16),
            pltpu.VMEM((CHUNKS * rows, 4 * depth), F32),
            pltpu.VMEM((3, CHUNKS * rows, out_width), F32),
            pltpu.VMEM((ny - 1, CHUNKS * rows, out_width), BF16),
            pltpu.VMEM((ny - 1, CHUNKS * rows, out_width), BF16),
            pltpu.VMEM((2, peers, 2, 384), BF16),
            pltpu.VMEM((2, peers, 2, 384), BF16),
            dma((4,)),
            dma((3,)),
            dma((3,)),
            dma((3,)),
            dma,
            dma((CHUNKS,)),
            dma,
            dma((3, CHUNKS)),
            dma,
            dma((ny - 1, CHUNKS)),
            dma((4,)),
            dma((2, CHUNKS + 1)),
        ],
        compiler_params=pltpu.CompilerParams(collective_id=0, has_side_effects=True),
    )(
        tokens,
        norm_gain.reshape(1, width),
        routing.T,
        route_weight.T,
        w_gate[0].T,
        w_up[0].T,
        w_down.reshape(depth, width),
    )


def solution(mesh):
    placed = (
        P("ep", None),
        P(),
        P("ep", None),
        P("ep", None),
        P("ep", None, "tp"),
        P("ep", None, "tp"),
        P("ep", "tp", None),
    )
    body = functools.partial(local, mesh.shape["ep"] // NX, mesh.shape["tp"] // 2)
    return jax.shard_map(body, mesh=mesh, in_specs=placed, out_specs=P("ep", "tp"), check_vma=False)
```

```python
import functools

import jax
import jax.numpy as jnp
from jax import lax
from jax.experimental import pallas as pl
from jax.experimental.pallas import tpu as pltpu
from jax.sharding import PartitionSpec as P

NORM_EPS = 1e-06
CLAMP_LIMIT = 7.0
SIGMOID_SCALE = 1.702
MESH = pl.DeviceIdType.MESH
NX = 4
CHUNKS = 3
SHARES = 4
F32 = jnp.float32
BF16 = jnp.bfloat16


def dot(a, b):
    return jnp.dot(a, b, preferred_element_type=F32)


def kernel(
    nz, ny, tok_hbm, gain_hbm, route_hbm, rw_hbm, wg_ref, wu_ref, wd_ref, out_ref,
    tok_ref, gain_ref, route_ref, rw_ref, guw, dw, packed, spilled, gathered, sbuf, rbuf, xs, acc, own, ssend, srecv, rsend, rret,
    in_sem, w_sem, wp_send, wp_recv, d_send, d_recv, y_send, y_recv, s_send, s_recv, r_send, r_recv,
):
    ep, tp = lax.axis_index("ep"), lax.axis_index("tp")
    z, x = lax.div(ep, NX), lax.rem(ep, NX)
    y, core = lax.div(tp, 2), lax.rem(tp, 2)
    other = 1 - core
    toks, depth = tok_ref.shape[0], wd_ref.shape[0]
    peers = sbuf.shape[0]
    per = peers // CHUNKS
    half = xs.shape[2] // 2
    share = 2 * half
    lanes = out_ref.shape[1]

    def dev(dz, dx, dy, at):
        return (
            lax.rem(z + dz + 2 * nz, nz) * NX + lax.rem(x + dx + NX, NX),
            lax.rem(y + dy + ny, ny) * 2 + at,
        )

    def offset(j, sender):
        return nz // 4 + sender * (nz // 2) + j // NX, (j + 1) % NX

    def remote(src, dst, send, recv, to):
        return pltpu.make_async_remote_copy(
            src_ref=src, dst_ref=dst, send_sem=send, recv_sem=recv, device_id=to, device_id_type=MESH
        )

    partner = dev(0, 0, 0, other)
    def source(j, at):
        dz, dx = offset(j, other)
        return dev(-dz, -dx, 0, at)

    sources = [source(j, other) for j in range(peers)]
    targets = [dev(*offset(j, core), 0, other) for j in range(peers)]
    own_slot = peers // 2 + NX - 1
    chunk_order = (1, 2, 0)

    barrier = pltpu.get_barrier_semaphore()
    for to in sources + [dev(0, 0, dy, core) for dy in (2, -2, 1, -1)] + [partner]:
        pl.semaphore_signal(barrier, inc=1, device_id=to, device_id_type=MESH)

    fetches = [
        pltpu.make_async_copy(src, dst, in_sem.at[n])
        for n, (src, dst) in enumerate(
            ((tok_hbm, tok_ref), (gain_hbm, gain_ref), (route_hbm, route_ref), (rw_hbm, rw_ref))
        )
    ]
    for fetch in fetches:
        fetch.start()
    local = [
        pltpu.make_async_copy(wg_ref, guw.at[0], w_sem.at[0]),
        pltpu.make_async_copy(wu_ref, guw.at[2], w_sem.at[1]),
    ]
    for copy in local:
        copy.start()
    out_width = dw.shape[3]
    for q in range(ny):
        pltpu.make_async_copy(
            wd_ref.at[:, pl.ds(q * out_width, out_width)], dw.at[0, q], w_sem.at[2]
        ).start()

    for fetch in fetches:
        fetch.wait()
    values = tok_ref[...].astype(F32)
    scale = lax.rsqrt(jnp.mean(values * values, axis=-1, keepdims=True) + NORM_EPS)
    at = pl.multiple_of(lax.rem(y, SHARES) * share, 128)
    shared = tok_ref[:, pl.ds(at, share)].astype(F32)
    normal = (shared * scale * gain_ref[:, pl.ds(at, share)]).astype(BF16)

    routes, weights = route_ref[...], rw_ref[...]
    earlier = jnp.where(
        lax.broadcasted_iota(jnp.int32, (toks, toks), 0) < lax.broadcasted_iota(jnp.int32, (toks, toks), 1),
        1.0,
        0.0,
    ).astype(BF16)

    def named(sender, peer):
        ez = z + nz // 4 + sender * (nz // 2) + (peer >> 2)
        ez = jnp.where(ez >= nz, ez - nz, ez)
        ez = jnp.where(ez >= nz, ez - nz, ez)
        expert = ez * NX + ((x + peer + 1) & (NX - 1))
        hit = jnp.zeros((peer.shape[0], toks), F32)
        weight = jnp.zeros((peer.shape[0], toks), F32)
        for k in range(routes.shape[0]):
            same = routes[k : k + 1] == expert
            hit = hit + jnp.where(same, 1.0, 0.0)
            weight = weight + jnp.where(same, weights[k : k + 1], 0.0)
        return hit, weight, dot(hit.astype(BF16), earlier)

    row = lax.broadcasted_iota(jnp.int32, (peers * 2, 1), 0)
    hit, _, before = named(core, row >> 1)

    def pick(at, place):
        return jnp.where(((row & 1) == at) & (before == place), hit, 0.0).astype(BF16)

    first_half, second_half = normal[:, :half], normal[:, half:]
    upper_0, upper_1, lower_1, lower_2 = pick(0, 0.0), pick(0, 1.0), pick(1, 1.0), pick(1, 2.0)
    packed[:, pl.ds(0, half)] = dot(upper_0, first_half) + dot(lower_1, second_half)
    packed[:, pl.ds(half, half)] = dot(upper_0, second_half) + dot(lower_2, first_half)
    packed[:, pl.ds(share, half)] = dot(upper_1, first_half) + dot(lower_2, second_half)
    for j in range(peers):
        sbuf[j] = packed[pl.ds(2 * j, 2)].astype(BF16)

    pl.semaphore_wait(barrier, peers + 5)
    for j in [k * per + n for k in chunk_order for n in range(per)]:
        remote(sbuf.at[j], rbuf.at[j], d_send, d_recv.at[j // per], targets[j]).start()

    for copy in local:
        copy.wait()
    pltpu.make_async_copy(dw.at[0], dw.at[0], w_sem.at[2]).wait()
    pushes = [
        remote(src, dst, wp_send.at[n], wp_recv.at[n], partner)
        for n, (src, dst) in enumerate(
            ((guw.at[0], guw.at[1]), (guw.at[2], guw.at[3]), (dw.at[0], dw.at[1]))
        )
    ]
    for push in pushes:
        push.start()

    rows = per * 3
    to_row = lax.broadcasted_iota(jnp.int32, (rows, per * 6), 0)
    from_row = lax.broadcasted_iota(jnp.int32, (rows, per * 6), 1)
    third, block = (to_row * 11) >> 5, from_row >> 4
    meets = (((from_row & 15) >> 1) == third) & (block == to_row - 3 * third)
    first_c = jnp.where(meets & ((from_row & 1) == (block >> 1)), 1.0, 0.0).astype(BF16)
    second_c = jnp.where(meets & ((from_row & 1) == ((block + 1) >> 1)), 1.0, 0.0).astype(BF16)
    to_row = lax.broadcasted_iota(jnp.int32, (per * 6, rows), 0)
    from_row = lax.broadcasted_iota(jnp.int32, (per * 6, rows), 1)
    meets = from_row == 3 * ((to_row & 15) >> 1) + (to_row >> 4)
    first_e = jnp.where(meets & ((to_row & 1) == 0), 1.0, 0.0).astype(BF16)
    second_e = jnp.where(meets & ((to_row & 1) == 1), 1.0, 0.0).astype(BF16)

    row = lax.broadcasted_iota(jnp.int32, (peers * 12, 1), 0)
    place = jnp.where(row >= peers * 4, 1, 0) + jnp.where(row >= peers * 8, 1, 0)
    row = row - place * (peers * 4)
    holder = jnp.where(row >= peers * 2, 1, 0)
    hit, weight, before = named(1 - holder, (row - holder * (peers * 2)) >> 1)
    exact = jnp.where(before == place.astype(F32), hit * weight, 0.0).T
    lane_part = lax.broadcasted_iota(jnp.int32, exact.shape, 1) & 1
    mixing = []
    for part in range(2):
        kept = jnp.where(lane_part == part, exact, 0.0)
        high = kept.astype(BF16)
        mixing += [high, (kept - high.astype(F32)).astype(BF16)]
    mixing = jnp.concatenate(mixing, axis=0)

    spans = [pl.ds(g * rows, rows) for g in range(CHUNKS)]
    for g, k in enumerate(chunk_order):
        part = rbuf.at[pl.ds(k * per, per)]
        remote(part, part, d_send, d_recv.at[k], partner).wait_recv()
        for n in range(per):
            packed[pl.ds(2 * n, 2)] = rbuf[k * per + n].astype(F32)
        blocks = [packed[pl.ds(0, 2 * per), pl.ds(n * half, half)].astype(BF16) for n in range(3)]
        span = spans[g]
        xs[0, span, :half] = dot(first_c, jnp.concatenate([blocks[0], blocks[2], blocks[1]], axis=0)).astype(BF16)
        xs[0, span, half:] = dot(second_c, jnp.concatenate([blocks[1], blocks[0], blocks[2]], axis=0)).astype(BF16)
        whole = xs.at[0, span]
        left, right = xs.at[0, span, pl.ds(0, half)], xs.at[0, span, pl.ds(half, half)]
        remote(left, xs.at[3, span, pl.ds(0, half)], y_send, y_recv.at[2, g], dev(0, 0, 2, core)).start()
        remote(right, xs.at[3, span, pl.ds(half, half)], y_send, y_recv.at[2, g], dev(0, 0, -2, core)).start()
        remote(whole, xs.at[1, span], y_send, y_recv.at[0, g], dev(0, 0, 1, core)).start()
        remote(whole, xs.at[2, span], y_send, y_recv.at[1, g], dev(0, 0, -1, core)).start()

    for push in pushes:
        push.wait_recv()

    def products(block, dy):
        span = pl.ds(pl.multiple_of(lax.rem(y + dy + SHARES, SHARES) * share, 128), share)
        both = guw[:, :, span].reshape(4 * depth, share)
        return lax.dot_general(block, both, (((1,), (1,)), ((), ())), preferred_element_type=F32)

    acc[...] = products(xs[0], 0)

    def hidden_of(gs):
        span = pl.ds(gs[0] * rows, len(gs) * rows)
        sums = acc[span]
        for n, dy in ((1, -1), (2, 1), (3, 2)):
            for g in gs:
                part = xs.at[n, spans[g]]
                remote(part, part, y_send, y_recv.at[n - 1, g], partner).wait_recv()
            sums = sums + products(xs[n, span], dy)
        gated = jnp.minimum(sums[:, : 2 * depth], CLAMP_LIMIT)
        upper = jnp.clip(sums[:, 2 * depth :], -CLAMP_LIMIT, CLAMP_LIMIT)
        return ((upper + 1.0) * gated * jax.nn.sigmoid(SIGMOID_SCALE * gated)).astype(BF16)

    sign = 1 - 2 * core
    ahead, ahead2 = dev(0, 0, sign, core), dev(0, 0, 2 * sign, core)
    behind, behind2 = dev(0, 0, -sign, core), dev(0, 0, -2 * sign, core)

    def terms(hidden, steps):
        blocks = []
        for step in steps:
            to = lax.rem(y + step * sign + ny, ny)
            blocks.append(jnp.concatenate([dw[0, to], dw[1, to]], axis=0))
        out = dot(hidden, jnp.concatenate(blocks, axis=1))
        return [out[:, n * out_width : (n + 1) * out_width] for n in range(len(steps))]

    def ship(slot, g, value, to):
        ssend[slot, spans[g]] = value.astype(BF16)
        launch(slot, g, to)

    def launch(slot, g, to):
        remote(
            ssend.at[slot, spans[g]], srecv.at[slot, spans[g]], s_send, s_recv.at[slot, g], to
        ).start()

    def take(slot, g):
        part = srecv.at[slot, spans[g]]
        remote(part, part, s_send, s_recv.at[slot, g], partner).wait_recv()
        return part[...].astype(F32)

    def first_stage(gs, hidden):
        to_ship = ((0, 4, ahead2), (1, 3, ahead), (2, -3, behind))
        out = terms(hidden, [step for _, step, _ in to_ship] + [2])
        for n, g in enumerate(gs):
            for (slot, _, to), value in zip(to_ship, out):
                ship(slot, g, value[n * rows : (n + 1) * rows], to)
            own[0, spans[g]] = out[3][n * rows : (n + 1) * rows]
        out = terms(hidden, (-2, 0, 1, -1))
        for n, g in enumerate(gs):
            for slot, value in enumerate(out[:2]):
                own[slot + 1, spans[g]] = value[n * rows : (n + 1) * rows]
            for slot, value in enumerate(out[2:]):
                ssend[slot + 3, spans[g]] = value[n * rows : (n + 1) * rows].astype(BF16)

    def neighbours(g):
        launch(3, g, ahead)
        launch(4, g, behind)

    def relay(g):
        ship(5, g, own[0, spans[g]] + take(0, g) + take(1, g), ahead2)
        ship(6, g, own[1, spans[g]] + take(2, g), behind2)

    is_0 = core == 0
    lane = 128
    own_chip = remote(
        rsend.at[0, own_slot], rret.at[core, own_slot], r_send.at[3], r_recv.at[0, CHUNKS], source(own_slot, core)
    )

    def give_back(g):
        total = own[2, spans[g]]
        for slot in (3, 4, 6, 5):
            total = total + take(slot, g)
        total = total.astype(BF16)
        ends, middle = dot(first_e, total), dot(second_e, total[:, lane : 2 * lane])
        first_slot = chunk_order[g] * per
        spreads = []
        for spread in (ends[:, :lane] + middle, ends[:, 2 * lane :] + middle):
            spreads.append(jnp.concatenate([spread[n * 2 * per : (n + 1) * 2 * per] for n in range(3)], axis=1))
        spilled[0] = jnp.where(is_0, spreads[0], spreads[1])
        spilled[1] = jnp.where(is_0, spreads[1], spreads[0])
        for n in range(per):
            rsend[0, first_slot + n] = spilled[0, pl.ds(2 * n, 2)].astype(BF16)
            rsend[1, first_slot + n] = spilled[1, pl.ds(2 * n, 2)].astype(BF16)
        for j in range(first_slot, first_slot + per):
            remote(rsend.at[1, j], rret.at[core, j], r_send.at[1], r_recv.at[1, g], source(j, other)).start()
            if j != own_slot:
                to, half_send = source(j, core), r_send.at[0 if j < own_slot else 2]
                remote(rsend.at[0, j], rret.at[core, j], half_send, r_recv.at[0, g], to).start()
                continue

            @pl.when(core == 1)
            def _():
                own_chip.start()

            @pl.when(is_0)
            def _():
                rret[0, own_slot] = rsend[0, own_slot]

    for gs in ((0,), (1, 2)):
        first_stage(gs, hidden_of(gs))
        if gs == (0,):
            neighbours(0)
    for g in range(CHUNKS):
        relay(g)
        if g + 1 < CHUNKS:
            neighbours(g + 1)
    for g in range(CHUNKS):
        give_back(g)

    for g, k in enumerate(chunk_order):
        crossed = rret.at[other, pl.ds(k * per, per)]
        remote(crossed, crossed, d_send, r_recv.at[1, g], partner).wait_recv()
        holds_own = own_slot // per == k
        stayed = rret.at[core, pl.ds(k * per, per - 1 if holds_own else per)]
        remote(stayed, stayed, d_send, r_recv.at[0, g], partner).wait_recv()
        if holds_own:

            @pl.when(core == 1)
            def _():
                own_chip.wait_recv()

        for holder in range(2):
            for j in range(k * per, (k + 1) * per):
                gathered[pl.ds((holder * peers + j) * 2, 2)] = rret[holder, j].astype(F32)
    back = gathered[...].astype(BF16)
    back = jnp.concatenate([back[:, n * lane : (n + 1) * lane] for n in range(3)], axis=0)
    mixed = dot(mixing, back)
    ends = mixed[:toks] + mixed[toks : 2 * toks]
    middle = mixed[2 * toks : 3 * toks] + mixed[3 * toks :]
    out_0 = jnp.concatenate([ends, middle[:, : lanes - lane]], axis=1)
    out_1 = jnp.concatenate([middle[:, 2 * lane - lanes :], ends], axis=1)
    out_ref[...] = jnp.where(is_0, out_0, out_1).astype(BF16)

    remote(sbuf, rbuf, d_send, d_recv.at[0], partner).wait_send()
    for push in pushes:
        push.wait_send()
    others = xs.at[pl.ds(1, 3)]
    remote(others, others, y_send, d_recv.at[0], partner).wait_send()
    remote(ssend, srecv, s_send, d_recv.at[0], partner).wait_send()
    remote(rsend.at[1], rret.at[0], r_send.at[1], d_recv.at[0], partner).wait_send()
    for n, begin, count in ((0, 0, own_slot), (2, own_slot + 1, peers - 1 - own_slot)):
        stayed = rsend.at[0, pl.ds(begin, count)]
        remote(stayed, stayed, r_send.at[n], d_recv.at[0], partner).wait_send()

    @pl.when(core == 1)
    def _():
        own_chip.wait_send()


def local(nz, ny, tokens, norm_gain, routing, route_weight, w_gate, w_up, w_down):
    toks, width = tokens.shape
    depth = w_gate.shape[2]
    peers = nz * NX // 2
    per = peers // CHUNKS
    rows = per * 3
    share = width // SHARES
    half = share // 2
    out_width = width // ny
    vmem = functools.partial(pl.BlockSpec, memory_space=pltpu.VMEM)
    hbm = functools.partial(pl.BlockSpec, memory_space=pl.ANY)
    dma = pltpu.SemaphoreType.DMA
    return pl.pallas_call(
        functools.partial(kernel, nz, ny),
        out_shape=jax.ShapeDtypeStruct((toks, width // (2 * ny)), BF16),
        in_specs=[hbm()] * 7,
        out_specs=vmem(),
        scratch_shapes=[
            pltpu.VMEM((toks, width), BF16),
            pltpu.VMEM((1, width), F32),
            pltpu.VMEM(routing.shape[::-1], jnp.int32),
            pltpu.VMEM(routing.shape[::-1], F32),
            pltpu.VMEM((4, depth, width), BF16),
            pltpu.VMEM((2, ny, depth, out_width), BF16),
            pltpu.VMEM((peers * 2, 3 * half), F32),
            pltpu.VMEM((2, per * 2, 384), F32),
            pltpu.VMEM((peers * 4, 384), F32),
            pltpu.VMEM((peers, 2, 3 * half), BF16),
            pltpu.VMEM((peers, 2, 3 * half), BF16),
            pltpu.VMEM((SHARES, CHUNKS * rows, share), BF16),
            pltpu.VMEM((CHUNKS * rows, 4 * depth), F32),
            pltpu.VMEM((3, CHUNKS * rows, out_width), F32),
            pltpu.VMEM((ny - 1, CHUNKS * rows, out_width), BF16),
            pltpu.VMEM((ny - 1, CHUNKS * rows, out_width), BF16),
            pltpu.VMEM((2, peers, 2, 384), BF16),
            pltpu.VMEM((2, peers, 2, 384), BF16),
            dma((4,)),
            dma((3,)),
            dma((3,)),
            dma((3,)),
            dma,
            dma((CHUNKS,)),
            dma,
            dma((3, CHUNKS)),
            dma,
            dma((ny - 1, CHUNKS)),
            dma((4,)),
            dma((2, CHUNKS + 1)),
        ],
        compiler_params=pltpu.CompilerParams(collective_id=0, has_side_effects=True),
    )(
        tokens,
        norm_gain.reshape(1, width),
        routing.T,
        route_weight.T,
        w_gate[0].T,
        w_up[0].T,
        w_down.reshape(depth, width),
    )


def solution(mesh):
    placed = (
        P("ep", None),
        P(),
        P("ep", None),
        P("ep", None),
        P("ep", None, "tp"),
        P("ep", None, "tp"),
        P("ep", "tp", None),
    )
    body = functools.partial(local, mesh.shape["ep"] // NX, mesh.shape["tp"] // 2)
    return jax.shard_map(body, mesh=mesh, in_specs=placed, out_specs=P("ep", "tp"), check_vma=False)
```
